32 devices in a mesh: sp: 8 (over z, core), tp: 4 (over y, x).
Axes of the slice: x: 2, y: 2, z: 4, core: 2. Of those that a mesh axis runs over, the one named last changes fastest.
Arguments:
- tokens: bfloat16 [2, 6144, 4096], P(None, 'sp', 'tp'), may hold values from -6 to 6
- w_key: bfloat16 [4096, 2048], P(None, 'tp'), may hold values from -0.09375 to 0.09375
- w_value: bfloat16 [4096, 2048], P(None, 'tp'), may hold values from -0.09375 to 0.09375
- w_gate: bfloat16 [4096, 4, 16], replicated, may hold values from -0.09375 to 0.09375
- forget_bias: float32 [2, 16], replicated, may hold values from 3.9 to 13, as said below
- log_shift: float32 [2, 4, 16, 6144], P(None, None, 'tp', 'sp'), may hold values from -5 to 121, as said below
- new_query: bfloat16 [2, 1024, 2048], P(None, 'sp', 'tp'), may hold values from -6 to 6
Outputs:
- cache_matrix: bfloat16 [2, 2, 16, 128, 128], P(None, None, 'tp')
- cache_norm: float32 [2, 2, 16, 128], P(None, None, 'tp')
- cache_max: float32 [2, 2, 16], P(None, None, 'tp')
- first_read: bfloat16 [2, 1024, 2048], P(None, 'sp', 'tp')
The draws below stay inside these ranges and needn't reach their ends.
Inputs may be any that keep to these rules, and one draw needn't show every extreme that they name: `forget_bias`: added to the forget gates' pre-activations, by direction and head. `log_shift`: rows 0 and 2 are added to the input gates of the two directions; rows 1 and 3 are added to the log forget gates and are never positive.
All inputs are finite; a program needn't handle non-finite values.
Results may differ from the reference program's by a relative error of at most 0.024.
Values may be sent and summed in bfloat16 or wider, within the bound.
No kernel may reach another device: no remote copies, remote signals or barrier semaphores. Data moves between devices by JAX's collectives and lax.ppermute only.
A program may use at most 64 MiB of HBM per device.

```python
import math
import jax
import jax.numpy as jnp
from jax import lax

D = 4096
HEADS = 16
HEAD = 128
SEQS = 2
SEG = 768
CONTEXT_SPAN = 6144
NEW = 1024


def draw_forget_bias(key, part):
    pick_key, fast_key, slow_key = jax.random.split(jax.random.fold_in(key, 7), 3)
    slow_share = 0.5
    is_slow = jax.random.uniform(pick_key, (2, HEADS)) < slow_share
    fast_value = jax.random.uniform(fast_key, (2, HEADS), minval=3.9, maxval=5.0)
    slow_value = math.log(CONTEXT_SPAN) + 2.0 + jax.random.uniform(slow_key, (2, HEADS), minval=0.0, maxval=0.5)
    return jnp.where(is_slow, slow_value, fast_value).astype(jnp.float32)


def draw_log_shift(key, part):
    parallel_texts = jax.random.split(jax.random.fold_in(key, 13), 6)
    array_dimensions = (SEQS, 4, HEADS, CONTEXT_SPAN)
    inputs = jnp.clip(jax.random.normal(parallel_texts[0], array_dimensions), -4.0, 4.0)
    shrink_factor = jnp.exp(jax.random.uniform(parallel_texts[3], (SEQS, 1, HEADS, CONTEXT_SPAN // SEG), minval=math.log(0.25), maxval=0.0))
    shrink_factor = jnp.repeat(shrink_factor, SEG, axis=3)
    span_of_batch = jax.random.uniform(parallel_texts[4], array_dimensions) < 2.0 / CONTEXT_SPAN
    layer_stack_count = jax.random.uniform(parallel_texts[5], array_dimensions, minval=0.22, maxval=0.69)
    retention_switch = -shrink_factor / CONTEXT_SPAN - jnp.where(span_of_batch, layer_stack_count, 0.0)
    is_forget = (jnp.arange(4) % 2 == 1)[None, :, None, None]
    return jnp.where(is_forget, retention_switch, inputs).astype(jnp.float32)


def shard_levels(key, dims, cuts, least, top_value):
    gain, own = 1.0, jax.random.fold_in(key, 6)
    for dim, shards_of in cuts:
        steps = jnp.exp(jax.random.uniform(jax.random.fold_in(own, dim), (shards_of,), jnp.float32, least / len(cuts), top_value / len(cuts)))
        gain = gain * jnp.repeat(steps, dims[dim] // shards_of).reshape([-1 if axis == dim else 1 for axis in range(len(dims))])
    return gain


def scatter_about(rng, shape, spread, reach, cuts=(), kind=jnp.bfloat16):
    values = spread * jax.random.normal(rng, shape, jnp.float32)
    if cuts:
        values = values * shard_levels(rng, shape, cuts, -0.22, 0.18)
    return jnp.clip(values, -reach, reach).astype(kind)


def setup_inputs(seed: int = 0) -> dict:
    arg_keys = jax.random.split(jax.random.key(seed), 8)
    return {
        "tokens": scatter_about(arg_keys[0], (SEQS, CONTEXT_SPAN, D), 1.0, 6.0, ((1, 8), (2, 4))),
        "w_key": scatter_about(arg_keys[1], (D, HEADS * HEAD), D ** -0.5, 0.09375, ((1, 4),)),
        "w_value": scatter_about(arg_keys[2], (D, HEADS * HEAD), D ** -0.5, 0.09375, ((1, 4),)),
        "w_gate": scatter_about(arg_keys[3], (D, 4, HEADS), D ** -0.5, 0.09375),
        "forget_bias": draw_forget_bias(jax.random.fold_in(arg_keys[7], 71), 0),
        "log_shift": draw_log_shift(jax.random.fold_in(arg_keys[7], 71), 0),
        "new_query": scatter_about(arg_keys[6], (SEQS, NEW, HEADS * HEAD), 1.0, 6.0, ((1, 8), (2, 4))),
    }


def reference(tokens, w_key, w_value, w_gate, forget_bias, log_shift, new_query):
    flat_tokens = tokens.reshape(SEQS * CONTEXT_SPAN, D)
    key_rows = jnp.dot(flat_tokens, w_key, preferred_element_type=jnp.float32).astype(jnp.bfloat16)
    key_rows = key_rows.reshape(SEQS, CONTEXT_SPAN, HEADS, HEAD)
    value_rows = jnp.dot(flat_tokens, w_value, preferred_element_type=jnp.float32).astype(jnp.bfloat16)
    value_rows = value_rows.reshape(SEQS, CONTEXT_SPAN, HEADS, HEAD)
    gate_rows = jnp.dot(flat_tokens, w_gate.reshape(D, 4 * HEADS), preferred_element_type=jnp.float32)
    gate_rows = gate_rows.reshape(SEQS, CONTEXT_SPAN, 4, HEADS).transpose(0, 2, 3, 1)
    input_fwd = gate_rows[:, 0] + log_shift[:, 0]
    forget_fwd = jax.nn.log_sigmoid(gate_rows[:, 1] + forget_bias[0][None, :, None]) + log_shift[:, 1]
    input_bwd = gate_rows[:, 2] + log_shift[:, 2]
    forget_bwd = jax.nn.log_sigmoid(gate_rows[:, 3] + forget_bias[1][None, :, None]) + log_shift[:, 3]
    climb_fwd = jnp.cumsum(forget_fwd, axis=-1)
    total_fwd = climb_fwd[..., -1]
    weight_fwd = total_fwd[..., None] - climb_fwd + input_fwd
    climb_bwd = jnp.cumsum(forget_bwd, axis=-1)
    total_bwd = climb_bwd[..., -1]
    weight_bwd = climb_bwd - forget_bwd + input_bwd
    weights = jnp.stack([weight_fwd, weight_bwd], axis=1)
    totals = jnp.stack([total_fwd, total_bwd], axis=1)
    cache_max = jnp.maximum(totals, jnp.max(weights, axis=-1))
    scale_now = jnp.exp(weights - cache_max[..., None])
    key_f = key_rows.astype(jnp.float32).transpose(0, 2, 1, 3) * (HEAD ** -0.5)
    value_f = value_rows.astype(jnp.float32).transpose(0, 2, 1, 3)
    cache_norm = jnp.einsum('bjhl,bhld->bjhd', scale_now, key_f, precision=lax.Precision.HIGHEST)
    matrices = []
    for direction in range(2):
        weighted = scale_now[:, direction, :, :, None] * key_f
        matrices.append(jnp.einsum('bhld,bhle->bhde', weighted, value_f, precision=lax.Precision.HIGHEST))
    cache_matrix = jnp.stack(matrices, axis=1).astype(jnp.bfloat16)
    queries = new_query.reshape(SEQS, NEW, HEADS, HEAD).astype(jnp.float32)
    numerator = jnp.einsum('bthd,bjhde->bjthe', queries, cache_matrix.astype(jnp.float32))
    denominator = jnp.einsum('bthd,bjhd->bjth', queries, cache_norm, precision=lax.Precision.HIGHEST)
    divisor = jnp.maximum(jnp.abs(denominator), 1.0)
    first_read = jnp.sum(numerator / divisor[..., None], axis=1)
    first_read = first_read.reshape(SEQS, NEW, HEADS * HEAD).astype(jnp.bfloat16)
    return cache_matrix, cache_norm, cache_max, first_read
```

```python
import jax
import jax.numpy as jnp
from jax import lax
from jax.experimental import pallas as pl
from jax.experimental.pallas import tpu as pltpu
from jax.sharding import PartitionSpec as P

HEAD = 128
SLAB = HEAD + 8
WIRE = HEAD + 16


def combined_all(array, axis, combine):
    everything = jax.tree.map(lambda part: lax.all_gather(part, axis), array)
    leading = jax.tree.map(lambda part: part[0], everything)

    def lap(k, so_far):
        return combine(so_far, jax.tree.map(lambda part: part[k], everything))

    return lax.fori_loop(1, lax.axis_size(axis), lap, leading)


def joint_max(earlier, latter):
    memory_a, norm_a, high_a = earlier
    memory_b, norm_b, high_b = latter
    highest = jnp.maximum(high_a, high_b)
    carried = jnp.exp(high_a - highest)
    own_part = jnp.exp(high_b - highest)
    memory = memory_a * carried[..., None, None] + memory_b * own_part[..., None, None]
    norm_sum = norm_a * carried[..., None] + norm_b * own_part[..., None]
    return (memory, norm_sum, highest)


def any_mesh(tokens, w_key, w_value, w_gate, forget_bias, log_shift, new_query):
    seq_count, seg_len, part_width = tokens.shape
    per_head = w_key.shape[1] // HEAD
    row_count = seq_count * seg_len
    first_head = lax.axis_index("tp") * per_head
    gate_cols = lax.dynamic_slice_in_dim(w_gate, first_head, per_head, 2).reshape(
        w_gate.shape[0], 4 * per_head
    )
    bias_own = lax.dynamic_slice_in_dim(forget_bias, first_head, per_head, 1)
    piece = lax.all_gather(tokens, "tp", axis=2, tiled=True)
    piece_width = piece.shape[2]
    flat_piece = piece.reshape(row_count, piece_width)
    key_sum = jnp.dot(flat_piece, w_key, preferred_element_type=jnp.float32)
    value_sum = jnp.dot(flat_piece, w_value, preferred_element_type=jnp.float32)
    gate_sum = jnp.dot(flat_piece, gate_cols, preferred_element_type=jnp.float32)
    key_rows = key_sum.astype(jnp.bfloat16).reshape(seq_count, seg_len, per_head, HEAD)
    value_rows = value_sum.astype(jnp.bfloat16).reshape(seq_count, seg_len, per_head, HEAD)
    gates = gate_sum.reshape(seq_count, seg_len, 4, per_head).transpose(0, 2, 3, 1)
    weights, totals = decay(gates, bias_own, log_shift)
    local_top = jnp.max(weights, axis=-1)
    scale_now = jnp.exp(weights - local_top[..., None])
    key_f = key_rows.astype(jnp.float32).transpose(0, 2, 1, 3) * HEAD ** (-0.5)
    value_f = value_rows.astype(jnp.float32).transpose(0, 2, 1, 3)
    weighted = scale_now[..., None] * key_f[:, None]
    memory = jnp.einsum("bjhld,bhle->bjhde", weighted, value_f, precision=lax.Precision.HIGHEST)
    norm_sum = jnp.sum(weighted, axis=3)
    every_total = lax.all_gather(totals[None], "sp", axis=0, tiled=True)
    my_index = lax.axis_index("sp")
    sources = jnp.arange(every_total.shape[0])[:, None, None, None]
    direction = jnp.arange(2)[None, None, :, None]
    counted = jnp.where(direction == 0, sources > my_index, sources < my_index)
    passed = jnp.sum(jnp.where(counted, every_total, 0.0), axis=0)
    total_all = jnp.sum(every_total, axis=0)
    memory_all, norm_all, top_all = combined_all(
        (memory, norm_sum, local_top + passed), "sp", joint_max
    )
    cache_max = jnp.maximum(total_all, top_all)
    rescale = jnp.exp(top_all - cache_max)
    cache_matrix = (memory_all * rescale[..., None, None]).astype(jnp.bfloat16)
    cache_norm = norm_all * rescale[..., None]
    new_count = new_query.shape[1]
    queries = new_query.reshape(seq_count, new_count, per_head, HEAD)
    numerator = jnp.einsum(
        "bthd,bjhde->bjthe", queries, cache_matrix, preferred_element_type=jnp.float32
    )
    denominator = jnp.einsum(
        "bthd,bjhd->bjth", queries.astype(jnp.float32), cache_norm, precision=lax.Precision.HIGHEST
    )
    divisor = jnp.maximum(jnp.abs(denominator), 1.0)
    first_read = jnp.sum(numerator / divisor[..., None], axis=1)
    first_read = first_read.reshape(seq_count, new_count, per_head * HEAD).astype(jnp.bfloat16)
    return (cache_matrix, cache_norm, cache_max, first_read)


def decay(gates, bias_own, log_shift):
    input_fwd = gates[:, 0] + log_shift[:, 0]
    forget_fwd = jax.nn.log_sigmoid(gates[:, 1] + bias_own[0][None, :, None]) + log_shift[:, 1]
    input_bwd = gates[:, 2] + log_shift[:, 2]
    forget_bwd = jax.nn.log_sigmoid(gates[:, 3] + bias_own[1][None, :, None]) + log_shift[:, 3]
    climb = jnp.cumsum(jnp.stack([forget_fwd, forget_bwd], axis=1), axis=-1)
    totals = climb[..., -1]
    weight_fwd = totals[:, 0, :, None] - climb[:, 0] + input_fwd
    weight_bwd = climb[:, 1] - forget_bwd + input_bwd
    return jnp.stack([weight_fwd, weight_bwd], axis=1), totals


def swap(array, axis, bit):
    size = lax.axis_size(axis)
    return lax.ppermute(array, axis, [(i, i ^ bit) for i in range(size)])


def z_shift(array, step):
    size = lax.axis_size("sp")
    return lax.ppermute(array, "sp", [(i, (i + 2 * step) % size) for i in range(size)])


def early_kernel(feature, own, over_x, over_y, *rest):
    weights, acc = rest[:6], rest[6]
    total = None
    for tokens, w_k, w_v in zip((own, over_x, over_y), weights[:3], weights[3:]):
        both = jnp.concatenate([w_k[...], w_v[...]], axis=1)
        part = jnp.dot(tokens[...], both, preferred_element_type=jnp.float32)
        total = part if total is None else total + part
    acc[...] = total


def early_projection(seq, feature, tokens, over_x, over_y, w_key, w_value):
    _, seg_len, width = tokens.shape
    per_head = w_key.shape[1] // HEAD

    def part(j):
        return pl.BlockSpec((width, HEAD), lambda h, f: (f[j], h))

    whole = pl.BlockSpec((seg_len, width), lambda h, f: (0, 0))
    return pl.pallas_call(
        early_kernel,
        grid_spec=pltpu.PrefetchScalarGridSpec(
            num_scalar_prefetch=1,
            grid=(per_head,),
            in_specs=[pl.BlockSpec((None, seg_len, width), lambda h, f: (seq, 0, 0)), whole, whole]
            + [part(j) for j in range(3)] * 2,
            out_specs=pl.BlockSpec((None, seg_len, 2 * HEAD), lambda h, f: (h, 0, 0)),
        ),
        out_shape=jax.ShapeDtypeStruct((per_head, seg_len, 2 * HEAD), jnp.float32),
        cost_estimate=pl.CostEstimate(
            flops=2 * seg_len * 3 * width * per_head * 2 * HEAD, bytes_accessed=0, transcendentals=0
        ),
        name="early",
    )(feature, tokens, over_x, over_y, w_key, w_key, w_key, w_value, w_value, w_value)


def late_kernel(feature, acc, far_a, far_b, w_k, w_v, scale, out):
    half = far_a.shape[0]
    both = jnp.concatenate([w_k[...], w_v[...]], axis=1)
    memory, norm = None, None
    for r, far in enumerate((far_a, far_b)):
        rows = pl.ds(r * half, half)
        kv = acc[rows, :] + jnp.dot(far[...], both, preferred_element_type=jnp.float32)
        kv = kv.astype(jnp.bfloat16)
        keys = kv[:, :HEAD].astype(jnp.float32)
        values = kv[:, HEAD:]
        now = scale[:, rows]
        keys_t = keys.T
        weighted = jnp.concatenate([keys_t * now[0:1], keys_t * now[1:2]], axis=0)
        part = jnp.dot(weighted.astype(jnp.bfloat16), values, preferred_element_type=jnp.float32)
        some = jnp.dot(now, keys, preferred_element_type=jnp.float32, precision=lax.Precision.HIGHEST)
        memory = part if memory is None else memory + part
        norm = some if norm is None else norm + some
    for j in range(2):
        out[j, :HEAD, :] = memory[j * HEAD : (j + 1) * HEAD]
        out[j, HEAD:, :] = jnp.broadcast_to(norm[j : j + 1], (SLAB - HEAD, HEAD))


def late_memory(feature, acc, far_a, far_b, w_key, w_value, scale):
    per_head, seg_len, _ = acc.shape
    half, width = far_a.shape
    part = pl.BlockSpec((width, HEAD), lambda h, f: (f[3], h))
    whole = pl.BlockSpec((half, width), lambda h, f: (0, 0))
    return pl.pallas_call(
        late_kernel,
        grid_spec=pltpu.PrefetchScalarGridSpec(
            num_scalar_prefetch=1,
            grid=(per_head,),
            in_specs=[
                pl.BlockSpec((None, seg_len, 2 * HEAD), lambda h, f: (h, 0, 0)),
                whole,
                whole,
                part,
                part,
                pl.BlockSpec((None, 8, seg_len), lambda h, f: (h, 0, 0)),
            ],
            out_specs=pl.BlockSpec((2, None, SLAB, HEAD), lambda h, f: (0, h, 0, 0)),
        ),
        out_shape=jax.ShapeDtypeStruct((2, per_head, SLAB, HEAD), jnp.float32),
        cost_estimate=pl.CostEstimate(
            flops=2 * seg_len * width * per_head * 2 * HEAD, bytes_accessed=0, transcendentals=0
        ),
        name="late",
    )(feature, acc, far_a, far_b, w_key, w_value, scale)


def to_wire(slab):
    matrix, norm = slab[..., :HEAD, :], slab[..., HEAD : HEAD + 1, :]
    high = norm.astype(jnp.bfloat16)
    low = (norm - high.astype(jnp.float32)).astype(jnp.bfloat16)
    rest = jnp.zeros(slab.shape[:-2] + (WIRE - HEAD - 2, HEAD), jnp.bfloat16)
    return jnp.concatenate([matrix.astype(jnp.bfloat16), high, low, rest], axis=-2)


def from_wire(wire):
    wire = wire.astype(jnp.float32)
    norm = wire[HEAD : HEAD + 1] + wire[HEAD + 1 : HEAD + 2]
    return jnp.concatenate([wire[:HEAD], jnp.broadcast_to(norm, (SLAB - HEAD, HEAD))], axis=0)


def read_kernel(place, *refs):
    seq_count, new_count, _ = refs[-4].shape
    slabs, query = refs[:-4], refs[-4]
    matrix_out, norm_out, read_out = refs[-3:]
    per_seq = len(slabs) // seq_count
    per_head = per_seq // 2
    core, chip = place[0], place[1]
    for b in range(seq_count):
        for i in range(per_seq):
            slab = slabs[b * per_seq + i]
            j = core if i < per_head else 1 - core
            h = lax.rem(chip + per_head - i % per_head, per_head)
            matrix_out[b, j, h] = slab[:HEAD, :]
            norm = slab[HEAD : HEAD + 8, :].astype(jnp.float32)
            norm_out[b, j, h] = jnp.broadcast_to(norm[0:1] + norm[1:2], (8, HEAD))
    for b in range(seq_count):
        for h in range(per_head):
            q = query[b, :, h * HEAD : (h + 1) * HEAD]
            q_f = q.astype(jnp.float32)
            total = None
            for j in range(2):
                top = jnp.dot(q, matrix_out[b, j, h], preferred_element_type=jnp.float32)
                below = jnp.sum(q_f * norm_out[b, j, h][0:1], axis=1, keepdims=True)
                part = top / jnp.maximum(jnp.abs(below), 1.0)
                total = part if total is None else total + part
            read_out[b, :, h * HEAD : (h + 1) * HEAD] = total.astype(jnp.bfloat16)


def assemble_and_read(place, slabs, query, per_head):
    seq_count, new_count, width = query.shape
    return pl.pallas_call(
        read_kernel,
        in_specs=[pl.BlockSpec(memory_space=pltpu.SMEM)]
        + [pl.BlockSpec(memory_space=pltpu.VMEM)] * (len(slabs) + 1),
        out_specs=[pl.BlockSpec(memory_space=pltpu.VMEM)] * 3,
        out_shape=[
            jax.ShapeDtypeStruct((seq_count, 2, per_head, HEAD, HEAD), jnp.bfloat16),
            jax.ShapeDtypeStruct((seq_count, 2, per_head, 8, HEAD), jnp.float32),
            jax.ShapeDtypeStruct((seq_count, new_count, width), jnp.bfloat16),
        ],
        name="read",
    )(place, *slabs, query)


def square_group(tokens, w_key, w_value, w_gate, forget_bias, log_shift, new_query):
    seq_count, seg_len, width = tokens.shape
    per_head = w_key.shape[1] // HEAD
    t = lax.axis_index("tp")
    s = lax.axis_index("sp")
    tp = lax.axis_size("tp")
    core, chip = s % 2, s // 2
    feature = jnp.stack([t, t ^ 1, t ^ 2, t ^ 3]).astype(jnp.int32)
    half = seg_len // 2

    over_x = [swap(tokens[b], "tp", 1) for b in range(seq_count)]
    over_y = [swap(tokens[b], "tp", 2) for b in range(seq_count)]
    far_a = [swap(over_x[b][:half], "tp", 2) for b in range(seq_count)]
    far_b = [swap(over_y[b][half:], "tp", 1) for b in range(seq_count)]

    gate_rows = lax.dynamic_slice_in_dim(w_gate, t * width, width, 0)
    gate_rows = gate_rows.reshape(width, 4, tp, per_head).transpose(2, 1, 3, 0)
    gate_part = lax.dot_general(
        gate_rows.reshape(tp * 4 * per_head, width),
        tokens.reshape(seq_count * seg_len, width),
        (((1,), (1,)), ((), ())),
        preferred_element_type=jnp.float32,
    ).reshape(tp, 4 * per_head, seq_count * seg_len)
    gates = lax.dynamic_index_in_dim(gate_part, t, 0, keepdims=False)
    for bit in range(1, tp):
        gates = gates + swap(lax.dynamic_index_in_dim(gate_part, t ^ bit, 0, keepdims=False), "tp", bit)
    gates = gates.reshape(4, per_head, seq_count, seg_len).transpose(2, 0, 1, 3)
    bias_own = lax.dynamic_slice_in_dim(forget_bias, t * per_head, per_head, 1)
    weights, totals = decay(gates, bias_own, log_shift)
    every = lax.all_gather(jnp.stack([totals, jnp.max(weights, axis=-1)]), "sp")
    every_total, every_top = every[:, 0], every[:, 1]
    sources = jnp.arange(every_total.shape[0])
    direction = jnp.arange(2)[None, None, None, :, None]
    later, sooner = sources[None, :] > sources[:, None], sources[None, :] < sources[:, None]
    counted = jnp.where(direction == 0, later[..., None, None, None], sooner[..., None, None, None])
    every_passed = jnp.sum(jnp.where(counted, every_total[None], 0.0), axis=1)
    cache_max = jnp.maximum(jnp.sum(every_total, axis=0), jnp.max(every_top + every_passed, axis=0))
    passed = lax.dynamic_index_in_dim(every_passed, s, 0, keepdims=False)
    scale = jnp.exp(weights + (passed - cache_max)[..., None]) * HEAD ** (-0.5)
    scale = scale.transpose(0, 2, 1, 3)
    scale = jnp.concatenate([scale, jnp.zeros((seq_count, per_head, 6, seg_len), jnp.float32)], axis=2)

    slabs = []
    for b in range(seq_count):
        acc = early_projection(b, feature, tokens, over_x[b], over_y[b], w_key, w_value)
        memory = late_memory(feature, acc, far_a[b], far_b[b], w_key, w_value, scale[b])
        other = swap(lax.dynamic_index_in_dim(memory, 1 - core, 0, keepdims=False), "sp", 1)
        mine = lax.dynamic_index_in_dim(memory, core, 0, keepdims=False) + other
        wire = to_wire(mine)
        own = lax.dynamic_index_in_dim(mine, chip, 0, keepdims=False)
        for step in range(1, per_head):
            part = lax.dynamic_index_in_dim(wire, (chip + step) % per_head, 0, keepdims=False)
            own = own + from_wire(z_shift(part, step))
        own = to_wire(own)
        row = [own] + [z_shift(own, step) for step in range(1, per_head)]
        slabs += row + [swap(part, "sp", 1) for part in row]

    place = jnp.stack([core, chip]).astype(jnp.int32)
    cache_matrix, norm, first_read = assemble_and_read(place, slabs, new_query, per_head)
    return (cache_matrix, norm[..., 0, :], cache_max, first_read)


def solution(mesh):
    def on_device(tokens, w_key, *rest):
        square = mesh.shape["tp"] == 4 and mesh.shape["sp"] == 2 * (w_key.shape[1] // HEAD)
        return (square_group if square else any_mesh)(tokens, w_key, *rest)

    return jax.shard_map(
        on_device,
        mesh=mesh,
        in_specs=(
            P(None, "sp", "tp"),
            P(None, "tp"),
            P(None, "tp"),
            P(),
            P(),
            P(None, None, "tp", "sp"),
            P(None, "sp", "tp"),
        ),
        out_specs=(
            P(None, None, "tp", None, None),
            P(None, None, "tp", None),
            P(None, None, "tp"),
            P(None, "sp", "tp"),
        ),
        check_vma=False,
    )
```

```python
import jax
import jax.numpy as jnp
from jax import lax
from jax.experimental import pallas as pl
from jax.experimental.pallas import tpu as pltpu
from jax.sharding import PartitionSpec as P


HEAD = 128
SLAB = HEAD + 8
WIRE = HEAD + 16


def combined_all(array, axis, combine):
    everything = jax.tree.map(lambda part: lax.all_gather(part, axis), array)
    leading = jax.tree.map(lambda part: part[0], everything)

    def lap(k, so_far):
        return combine(so_far, jax.tree.map(lambda part: part[k], everything))

    return lax.fori_loop(1, lax.axis_size(axis), lap, leading)


def joint_max(earlier, latter):
    memory_a, norm_a, high_a = earlier
    memory_b, norm_b, high_b = latter
    highest = jnp.maximum(high_a, high_b)
    carried = jnp.exp(high_a - highest)
    own_part = jnp.exp(high_b - highest)
    memory = memory_a * carried[..., None, None] + memory_b * own_part[..., None, None]
    norm_sum = norm_a * carried[..., None] + norm_b * own_part[..., None]
    return (memory, norm_sum, highest)


def any_mesh(tokens, w_key, w_value, w_gate, forget_bias, log_shift, new_query):
    seq_count, seg_len, _ = tokens.shape
    per_head = w_key.shape[1] // HEAD
    row_count = seq_count * seg_len
    first_head = lax.axis_index("tp") * per_head
    gate_cols = lax.dynamic_slice_in_dim(w_gate, first_head, per_head, 2).reshape(
        w_gate.shape[0], 4 * per_head
    )
    bias_own = lax.dynamic_slice_in_dim(forget_bias, first_head, per_head, 1)
    piece = lax.all_gather(tokens, "tp", axis=2, tiled=True)
    piece_width = piece.shape[2]
    flat_piece = piece.reshape(row_count, piece_width)
    key_sum = jnp.dot(flat_piece, w_key, preferred_element_type=jnp.float32)
    value_sum = jnp.dot(flat_piece, w_value, preferred_element_type=jnp.float32)
    gate_sum = jnp.dot(flat_piece, gate_cols, preferred_element_type=jnp.float32)
    key_rows = key_sum.astype(jnp.bfloat16).reshape(seq_count, seg_len, per_head, HEAD)
    value_rows = value_sum.astype(jnp.bfloat16).reshape(seq_count, seg_len, per_head, HEAD)
    gates = gate_sum.reshape(seq_count, seg_len, 4, per_head).transpose(0, 2, 3, 1)
    weights, totals = decay(gates, bias_own, log_shift)
    local_top = jnp.max(weights, axis=-1)
    scale_now = jnp.exp(weights - local_top[..., None])
    key_f = key_rows.astype(jnp.float32).transpose(0, 2, 1, 3) * HEAD ** (-0.5)
    value_f = value_rows.astype(jnp.float32).transpose(0, 2, 1, 3)
    weighted = scale_now[..., None] * key_f[:, None]
    memory = jnp.einsum("bjhld,bhle->bjhde", weighted, value_f, precision=lax.Precision.HIGHEST)
    norm_sum = jnp.sum(weighted, axis=3)
    every_total = lax.all_gather(totals[None], "sp", axis=0, tiled=True)
    my_index = lax.axis_index("sp")
    sources = jnp.arange(every_total.shape[0])[:, None, None, None]
    direction = jnp.arange(2)[None, None, :, None]
    counted = jnp.where(direction == 0, sources > my_index, sources < my_index)
    passed = jnp.sum(jnp.where(counted, every_total, 0.0), axis=0)
    total_all = jnp.sum(every_total, axis=0)
    memory_all, norm_all, top_all = combined_all(
        (memory, norm_sum, local_top + passed), "sp", joint_max
    )
    cache_max = jnp.maximum(total_all, top_all)
    rescale = jnp.exp(top_all - cache_max)
    cache_matrix = (memory_all * rescale[..., None, None]).astype(jnp.bfloat16)
    cache_norm = norm_all * rescale[..., None]
    new_count = new_query.shape[1]
    queries = new_query.reshape(seq_count, new_count, per_head, HEAD)
    numerator = jnp.einsum(
        "bthd,bjhde->bjthe", queries, cache_matrix, preferred_element_type=jnp.float32
    )
    denominator = jnp.einsum(
        "bthd,bjhd->bjth", queries.astype(jnp.float32), cache_norm, precision=lax.Precision.HIGHEST
    )
    divisor = jnp.maximum(jnp.abs(denominator), 1.0)
    first_read = jnp.sum(numerator / divisor[..., None], axis=1)
    first_read = first_read.reshape(seq_count, new_count, per_head * HEAD).astype(jnp.bfloat16)
    return (cache_matrix, cache_norm, cache_max, first_read)


def decay(gates, bias_own, log_shift):
    input_fwd = gates[:, 0] + log_shift[:, 0]
    forget_fwd = jax.nn.log_sigmoid(gates[:, 1] + bias_own[0][None, :, None]) + log_shift[:, 1]
    input_bwd = gates[:, 2] + log_shift[:, 2]
    forget_bwd = jax.nn.log_sigmoid(gates[:, 3] + bias_own[1][None, :, None]) + log_shift[:, 3]
    climb = jnp.cumsum(jnp.stack([forget_fwd, forget_bwd], axis=1), axis=-1)
    totals = climb[..., -1]
    weight_fwd = totals[:, 0, :, None] - climb[:, 0] + input_fwd
    weight_bwd = climb[:, 1] - forget_bwd + input_bwd
    return jnp.stack([weight_fwd, weight_bwd], axis=1), totals


def swap(array, axis, bit):
    size = lax.axis_size(axis)
    return lax.ppermute(array, axis, [(i, i ^ bit) for i in range(size)])


def early_kernel(feature, own, over_x, over_y, *rest):
    weights, acc = rest[:6], rest[6]
    total = None
    for tokens, w_k, w_v in zip((own, over_x, over_y), weights[:3], weights[3:]):
        both = jnp.concatenate([w_k[...], w_v[...]], axis=1)
        part = jnp.dot(tokens[...], both, preferred_element_type=jnp.float32)
        total = part if total is None else total + part
    acc[...] = total


def early_projection(seq, feature, tokens, over_x, over_y, w_key, w_value):
    _, seg_len, width = tokens.shape
    per_head = w_key.shape[1] // HEAD

    def part(j):
        return pl.BlockSpec((width, HEAD), lambda h, f: (f[j], h))

    whole = pl.BlockSpec((seg_len, width), lambda h, f: (0, 0))
    return pl.pallas_call(
        early_kernel,
        grid_spec=pltpu.PrefetchScalarGridSpec(
            num_scalar_prefetch=1,
            grid=(per_head,),
            in_specs=[pl.BlockSpec((None, seg_len, width), lambda h, f: (seq, 0, 0)), whole, whole]
            + [part(j) for j in range(3)] * 2,
            out_specs=pl.BlockSpec((None, seg_len, 2 * HEAD), lambda h, f: (h, 0, 0)),
        ),
        out_shape=jax.ShapeDtypeStruct((per_head, seg_len, 2 * HEAD), jnp.float32),
        cost_estimate=pl.CostEstimate(
            flops=2 * seg_len * 3 * width * per_head * 2 * HEAD, bytes_accessed=0, transcendentals=0
        ),
        name="early",
    )(feature, tokens, over_x, over_y, w_key, w_key, w_key, w_value, w_value, w_value)


def late_kernel(feature, acc, far_a, far_b, w_k, w_v, scale, keep, give):
    half = far_a.shape[0]
    both = jnp.concatenate([w_k[...], w_v[...]], axis=1)
    total = None
    for r, far in enumerate((far_a, far_b)):
        rows = pl.ds(r * half, half)
        kv = acc[rows, :] + jnp.dot(far[...], both, preferred_element_type=jnp.float32)
        kv = kv.astype(jnp.bfloat16)
        keys_t = kv[:, :HEAD].astype(jnp.float32).T
        now = scale[:, rows]
        high = now.astype(jnp.bfloat16)
        low = (now - high.astype(jnp.float32)).astype(jnp.bfloat16)
        left = jnp.concatenate(
            [
                (keys_t * now[0:1]).astype(jnp.bfloat16),
                (keys_t * now[1:2]).astype(jnp.bfloat16),
                jnp.concatenate([high, low], axis=0),
            ],
            axis=0,
        )
        part = jnp.dot(left, kv, preferred_element_type=jnp.float32)
        total = part if total is None else total + part
    slabs = []
    for j in range(2):
        norm = total[2 * HEAD + j : 2 * HEAD + j + 1, :HEAD]
        norm = norm + total[2 * HEAD + 8 + j : 2 * HEAD + 8 + j + 1, :HEAD]
        norm = jnp.broadcast_to(norm, (SLAB - HEAD, HEAD))
        slabs.append(jnp.concatenate([total[j * HEAD : (j + 1) * HEAD, HEAD:], norm], axis=0))
    first = feature[4] == 0
    keep[...] = jnp.where(first, slabs[0], slabs[1])
    give[...] = jnp.where(first, slabs[1], slabs[0])


def late_memory(feature, acc, far_a, far_b, w_key, w_value, scale):
    per_head, seg_len, _ = acc.shape
    half, width = far_a.shape
    part = pl.BlockSpec((width, HEAD), lambda h, f: (f[3], h))
    whole = pl.BlockSpec((half, width), lambda h, f: (0, 0))
    return pl.pallas_call(
        late_kernel,
        grid_spec=pltpu.PrefetchScalarGridSpec(
            num_scalar_prefetch=1,
            grid=(per_head,),
            in_specs=[
                pl.BlockSpec((None, seg_len, 2 * HEAD), lambda h, f: (h, 0, 0)),
                whole,
                whole,
                part,
                part,
                pl.BlockSpec((None, 8, seg_len), lambda h, f: (h, 0, 0)),
            ],
            out_specs=[pl.BlockSpec((None, SLAB, HEAD), lambda h, f: (h, 0, 0))] * 2,
        ),
        out_shape=[jax.ShapeDtypeStruct((per_head, SLAB, HEAD), jnp.float32)] * 2,
        cost_estimate=pl.CostEstimate(
            flops=2 * seg_len * width * per_head * 2 * HEAD, bytes_accessed=0, transcendentals=0
        ),
        name="late",
    )(feature, acc, far_a, far_b, w_key, w_value, scale)


def write_wire(out, matrix, norm):
    high = norm.astype(jnp.bfloat16).astype(jnp.float32)
    out[:, :HEAD, :] = matrix.astype(jnp.bfloat16)
    row = lax.broadcasted_iota(jnp.int32, (1, WIRE - HEAD, 1), 1)
    parts = jnp.where(row == 0, high, jnp.where(row == 1, norm - high, 0.0))
    out[:, HEAD:, :] = parts.astype(jnp.bfloat16)


def read_norm(wire):
    norm = wire[:, HEAD:, :].astype(jnp.float32)
    return norm[:, 0:1] + norm[:, 1:2]


def pack_kernel(mine, other, out):
    total = mine[...] + other[...]
    write_wire(out, total[:, :HEAD], total[:, HEAD : HEAD + 1])


def merge_kernel(mine, other, out):
    matrix = mine[:, :HEAD, :].astype(jnp.float32) + other[:, :HEAD, :].astype(jnp.float32)
    write_wire(out, matrix, read_norm(mine) + read_norm(other))


def joined(kernel, mine, other):
    return pl.pallas_call(
        kernel,
        in_specs=[pl.BlockSpec(memory_space=pltpu.VMEM)] * 2,
        out_specs=pl.BlockSpec(memory_space=pltpu.VMEM),
        out_shape=jax.ShapeDtypeStruct((mine.shape[0], WIRE, HEAD), jnp.bfloat16),
        name="join",
    )(mine, other)


def tie(array, *others):
    return lax.optimization_barrier((array,) + others)[0]


def add_over_sp(keep, give):
    wire = joined(pack_kernel, keep, swap(give, "sp", 1))
    bit = 2
    while bit < lax.axis_size("sp"):
        wire = joined(merge_kernel, wire, swap(wire, "sp", bit))
        bit *= 2
    return wire


def read_kernel(place, *refs):
    seq_count, _, _ = refs[-4].shape
    slabs, query = refs[:-4], refs[-4]
    matrix_out, norm_out, read_out = refs[-3:]
    per_head = matrix_out.shape[2]
    core = place[0]
    for b in range(seq_count):
        for i in range(2):
            slab = slabs[2 * b + i]
            j = core if i == 0 else 1 - core
            for h in range(per_head):
                matrix_out[b, j, h] = slab[h, :HEAD, :]
                norm_out[b, j, h] = jnp.broadcast_to(read_norm(slab[h : h + 1])[0], (8, HEAD))
    for b in range(seq_count):
        for h in range(per_head):
            q = query[b, :, h * HEAD : (h + 1) * HEAD]
            q_f = q.astype(jnp.float32)
            total = None
            for j in range(2):
                top = jnp.dot(q, matrix_out[b, j, h], preferred_element_type=jnp.float32)
                below = jnp.sum(q_f * norm_out[b, j, h][0:1], axis=1, keepdims=True)
                part = top / jnp.maximum(jnp.abs(below), 1.0)
                total = part if total is None else total + part
            read_out[b, :, h * HEAD : (h + 1) * HEAD] = total.astype(jnp.bfloat16)


def assemble_and_read(place, slabs, query, per_head):
    seq_count, new_count, width = query.shape
    return pl.pallas_call(
        read_kernel,
        in_specs=[pl.BlockSpec(memory_space=pltpu.SMEM)]
        + [pl.BlockSpec(memory_space=pltpu.VMEM)] * (len(slabs) + 1),
        out_specs=[pl.BlockSpec(memory_space=pltpu.VMEM)] * 3,
        out_shape=[
            jax.ShapeDtypeStruct((seq_count, 2, per_head, HEAD, HEAD), jnp.bfloat16),
            jax.ShapeDtypeStruct((seq_count, 2, per_head, 8, HEAD), jnp.float32),
            jax.ShapeDtypeStruct((seq_count, new_count, width), jnp.bfloat16),
        ],
        name="read",
    )(place, *slabs, query)


def square_group(tokens, w_key, w_value, w_gate, forget_bias, log_shift, new_query):
    seq_count, seg_len, width = tokens.shape
    per_head = w_key.shape[1] // HEAD
    t = lax.axis_index("tp")
    s = lax.axis_index("sp")
    tp = lax.axis_size("tp")
    core = s % 2
    feature = jnp.stack([t, t ^ 1, t ^ 2, t ^ 3, core]).astype(jnp.int32)
    half = seg_len // 2

    over_x = [swap(tokens[0], "tp", 1)]
    over_y = [swap(tokens[0], "tp", 2)]

    gate_rows = lax.dynamic_slice_in_dim(w_gate, t * width, width, 0)
    gate_rows = gate_rows.reshape(width, 4, tp, per_head).transpose(2, 1, 3, 0)
    gate_part = lax.dot_general(
        gate_rows.reshape(tp * 4 * per_head, width),
        tokens.reshape(seq_count * seg_len, width),
        (((1,), (1,)), ((), ())),
        preferred_element_type=jnp.float32,
    ).reshape(tp, 4 * per_head, seq_count * seg_len)
    shares = [
        swap(lax.dynamic_index_in_dim(gate_part, t ^ bit, 0, keepdims=False), "tp", bit)
        for bit in range(1, tp)
    ]
    for b in range(1, seq_count):
        ready = tie(tokens[b], gate_part)
        over_x.append(swap(ready, "tp", 1))
        over_y.append(swap(ready, "tp", 2))
    far_a, far_b, first = [], [], []
    for b in range(seq_count):
        first.append((over_x[b][:half], over_y[b][half:]))
        far_a.append(swap(first[b][0], "tp", 2))
        far_b.append(swap(first[b][1], "tp", 1))
    shares = lax.optimization_barrier(tuple(shares) + first[0])[: tp - 1]
    gates = lax.dynamic_index_in_dim(gate_part, t, 0, keepdims=False)
    for share in shares:
        gates = gates + share
    gates = gates.reshape(4, per_head, seq_count, seg_len).transpose(2, 0, 1, 3)
    bias_own = lax.dynamic_slice_in_dim(forget_bias, t * per_head, per_head, 1)
    weights, totals = decay(gates, bias_own, log_shift)
    every = lax.all_gather(jnp.stack([totals, jnp.max(weights, axis=-1)]), "sp")
    every_total, every_top = every[:, 0], every[:, 1]
    sources = jnp.arange(every_total.shape[0])
    direction = jnp.arange(2)[None, None, None, :, None]
    later, sooner = sources[None, :] > sources[:, None], sources[None, :] < sources[:, None]
    counted = jnp.where(direction == 0, later[..., None, None, None], sooner[..., None, None, None])
    every_passed = jnp.sum(jnp.where(counted, every_total[None], 0.0), axis=1)
    cache_max = jnp.maximum(jnp.sum(every_total, axis=0), jnp.max(every_top + every_passed, axis=0))
    passed = lax.dynamic_index_in_dim(every_passed, s, 0, keepdims=False)
    scale = jnp.exp(weights + (passed - cache_max)[..., None]) * HEAD ** (-0.5)
    scale = scale.transpose(0, 2, 1, 3)
    scale = jnp.concatenate([scale, jnp.zeros((seq_count, per_head, 6, seg_len), jnp.float32)], axis=2)

    accs = [
        early_projection(b, feature, tokens, over_x[b], over_y[b], w_key, w_value)
        for b in range(seq_count)
    ]
    slabs = []
    for b in range(seq_count):
        ahead = first[b + 1] + (accs[b + 1],) if b + 1 < seq_count else tuple(slabs)
        last_a, last_b = tie(far_a[b], *ahead), tie(far_b[b], *ahead)
        keep, give = late_memory(feature, accs[b], last_a, last_b, w_key, w_value, scale[b])
        mine = add_over_sp(keep, give)
        slabs += [mine, swap(mine, "sp", 1)]

    place = core.astype(jnp.int32)[None]
    cache_matrix, norm, first_read = assemble_and_read(place, slabs, new_query, per_head)
    return (cache_matrix, norm[..., 0, :], cache_max, first_read)


def solution(mesh):
    def on_device(tokens, w_key, *rest):
        square = mesh.shape["tp"] == 4 and mesh.shape["sp"] == 2 * (w_key.shape[1] // HEAD)
        return (square_group if square else any_mesh)(tokens, w_key, *rest)

    return jax.shard_map(
        on_device,
        mesh=mesh,
        in_specs=(
            P(None, "sp", "tp"),
            P(None, "tp"),
            P(None, "tp"),
            P(),
            P(),
            P(None, None, "tp", "sp"),
            P(None, "sp", "tp"),
        ),
        out_specs=(
            P(None, None, "tp", None, None),
            P(None, None, "tp", None),
            P(None, None, "tp"),
            P(None, "sp", "tp"),
        ),
        check_vma=False,
    )
```

```python
import jax
import jax.numpy as jnp
from jax import lax
from jax.experimental import pallas as pl
from jax.experimental.pallas import tpu as pltpu
from jax.sharding import PartitionSpec as P


HEAD = 128
SLAB = HEAD + 8


def combined_all(array, axis, combine):
    everything = jax.tree.map(lambda part: lax.all_gather(part, axis), array)
    leading = jax.tree.map(lambda part: part[0], everything)

    def lap(k, so_far):
        return combine(so_far, jax.tree.map(lambda part: part[k], everything))

    return lax.fori_loop(1, lax.axis_size(axis), lap, leading)


def joint_max(earlier, latter):
    memory_a, norm_a, high_a = earlier
    memory_b, norm_b, high_b = latter
    highest = jnp.maximum(high_a, high_b)
    carried = jnp.exp(high_a - highest)
    own_part = jnp.exp(high_b - highest)
    memory = memory_a * carried[..., None, None] + memory_b * own_part[..., None, None]
    norm_sum = norm_a * carried[..., None] + norm_b * own_part[..., None]
    return (memory, norm_sum, highest)


def any_mesh(tokens, w_key, w_value, w_gate, forget_bias, log_shift, new_query):
    seq_count, seg_len, _ = tokens.shape
    per_head = w_key.shape[1] // HEAD
    row_count = seq_count * seg_len
    first_head = lax.axis_index("tp") * per_head
    gate_cols = lax.dynamic_slice_in_dim(w_gate, first_head, per_head, 2).reshape(
        w_gate.shape[0], 4 * per_head
    )
    bias_own = lax.dynamic_slice_in_dim(forget_bias, first_head, per_head, 1)
    piece = lax.all_gather(tokens, "tp", axis=2, tiled=True)
    piece_width = piece.shape[2]
    flat_piece = piece.reshape(row_count, piece_width)
    key_sum = jnp.dot(flat_piece, w_key, preferred_element_type=jnp.float32)
    value_sum = jnp.dot(flat_piece, w_value, preferred_element_type=jnp.float32)
    gate_sum = jnp.dot(flat_piece, gate_cols, preferred_element_type=jnp.float32)
    key_rows = key_sum.astype(jnp.bfloat16).reshape(seq_count, seg_len, per_head, HEAD)
    value_rows = value_sum.astype(jnp.bfloat16).reshape(seq_count, seg_len, per_head, HEAD)
    gates = gate_sum.reshape(seq_count, seg_len, 4, per_head).transpose(0, 2, 3, 1)
    weights, totals = decay(gates, bias_own, log_shift)
    local_top = jnp.max(weights, axis=-1)
    scale_now = jnp.exp(weights - local_top[..., None])
    key_f = key_rows.astype(jnp.float32).transpose(0, 2, 1, 3) * HEAD ** (-0.5)
    value_f = value_rows.astype(jnp.float32).transpose(0, 2, 1, 3)
    weighted = scale_now[..., None] * key_f[:, None]
    memory = jnp.einsum("bjhld,bhle->bjhde", weighted, value_f, precision=lax.Precision.HIGHEST)
    norm_sum = jnp.sum(weighted, axis=3)
    every_total = lax.all_gather(totals[None], "sp", axis=0, tiled=True)
    my_index = lax.axis_index("sp")
    sources = jnp.arange(every_total.shape[0])[:, None, None, None]
    direction = jnp.arange(2)[None, None, :, None]
    counted = jnp.where(direction == 0, sources > my_index, sources < my_index)
    passed = jnp.sum(jnp.where(counted, every_total, 0.0), axis=0)
    total_all = jnp.sum(every_total, axis=0)
    memory_all, norm_all, top_all = combined_all(
        (memory, norm_sum, local_top + passed), "sp", joint_max
    )
    cache_max = jnp.maximum(total_all, top_all)
    rescale = jnp.exp(top_all - cache_max)
    cache_matrix = (memory_all * rescale[..., None, None]).astype(jnp.bfloat16)
    cache_norm = norm_all * rescale[..., None]
    new_count = new_query.shape[1]
    queries = new_query.reshape(seq_count, new_count, per_head, HEAD)
    numerator = jnp.einsum(
        "bthd,bjhde->bjthe", queries, cache_matrix, preferred_element_type=jnp.float32
    )
    denominator = jnp.einsum(
        "bthd,bjhd->bjth", queries.astype(jnp.float32), cache_norm, precision=lax.Precision.HIGHEST
    )
    divisor = jnp.maximum(jnp.abs(denominator), 1.0)
    first_read = jnp.sum(numerator / divisor[..., None], axis=1)
    first_read = first_read.reshape(seq_count, new_count, per_head * HEAD).astype(jnp.bfloat16)
    return (cache_matrix, cache_norm, cache_max, first_read)


def decay(gates, bias_own, log_shift):
    input_fwd = gates[:, 0] + log_shift[:, 0]
    forget_fwd = jax.nn.log_sigmoid(gates[:, 1] + bias_own[0][None, :, None]) + log_shift[:, 1]
    input_bwd = gates[:, 2] + log_shift[:, 2]
    forget_bwd = jax.nn.log_sigmoid(gates[:, 3] + bias_own[1][None, :, None]) + log_shift[:, 3]
    climb = jnp.cumsum(jnp.stack([forget_fwd, forget_bwd], axis=1), axis=-1)
    totals = climb[..., -1]
    weight_fwd = totals[:, 0, :, None] - climb[:, 0] + input_fwd
    weight_bwd = climb[:, 1] - forget_bwd + input_bwd
    return jnp.stack([weight_fwd, weight_bwd], axis=1), totals


def swap(array, axis, bit):
    size = lax.axis_size(axis)
    return lax.ppermute(array, axis, [(i, i ^ bit) for i in range(size)])


def early_kernel(feature, own, x_a, x_b, y_a, y_b, *rest):
    weights, acc = rest[:6], rest[6]
    half = x_a.shape[0]
    pairs = [jnp.concatenate([weights[j][...], weights[3 + j][...]], axis=1) for j in range(3)]
    for r, (over_x, over_y) in enumerate(((x_a, y_a), (x_b, y_b))):
        rows = pl.ds(r * half, half)
        total = jnp.dot(own[rows, :], pairs[0], preferred_element_type=jnp.float32)
        total += jnp.dot(over_x[...], pairs[1], preferred_element_type=jnp.float32)
        total += jnp.dot(over_y[...], pairs[2], preferred_element_type=jnp.float32)
        acc[rows, :] = total


def early_projection(seq, feature, tokens, blocks, w_key, w_value):
    _, seg_len, width = tokens.shape
    per_head = w_key.shape[1] // HEAD
    half = seg_len // 2

    def part(j):
        return pl.BlockSpec((width, HEAD), lambda h, f: (f[j], h))

    whole = pl.BlockSpec((half, width), lambda h, f: (0, 0))
    return pl.pallas_call(
        early_kernel,
        grid_spec=pltpu.PrefetchScalarGridSpec(
            num_scalar_prefetch=1,
            grid=(per_head,),
            in_specs=[pl.BlockSpec((None, seg_len, width), lambda h, f: (seq, 0, 0))]
            + [whole] * 4
            + [part(j) for j in range(3)] * 2,
            out_specs=pl.BlockSpec((None, seg_len, 2 * HEAD), lambda h, f: (h, 0, 0)),
        ),
        out_shape=jax.ShapeDtypeStruct((per_head, seg_len, 2 * HEAD), jnp.float32),
        cost_estimate=pl.CostEstimate(
            flops=2 * seg_len * 3 * width * per_head * 2 * HEAD, bytes_accessed=0, transcendentals=0
        ),
        compiler_params=pltpu.CompilerParams(vmem_limit_bytes=24 << 20),
        name="early",
    )(feature, tokens, *blocks, w_key, w_key, w_key, w_value, w_value, w_value)


def late_kernel(feature, acc, far_a, far_b, w_k, w_v, scale, keep, give):
    half = far_a.shape[0]
    both = jnp.concatenate([w_k[...], w_v[...]], axis=1)
    total = None
    for r, far in enumerate((far_a, far_b)):
        rows = pl.ds(r * half, half)
        kv = acc[rows, :] + jnp.dot(far[...], both, preferred_element_type=jnp.float32)
        kv = kv.astype(jnp.bfloat16)
        keys_t = kv[:, :HEAD].astype(jnp.float32).T
        now = scale[:, rows]
        high = now.astype(jnp.bfloat16)
        low = (now - high.astype(jnp.float32)).astype(jnp.bfloat16)
        left = jnp.concatenate(
            [
                (keys_t * now[0:1]).astype(jnp.bfloat16),
                (keys_t * now[1:2]).astype(jnp.bfloat16),
                jnp.concatenate([high, low], axis=0),
            ],
            axis=0,
        )
        part = jnp.dot(left, kv, preferred_element_type=jnp.float32)
        total = part if total is None else total + part
    slabs = []
    for j in range(2):
        norm = total[2 * HEAD + j : 2 * HEAD + j + 1, :HEAD]
        norm = norm + total[2 * HEAD + 8 + j : 2 * HEAD + 8 + j + 1, :HEAD]
        norm = jnp.broadcast_to(norm, (SLAB - HEAD, HEAD))
        slabs.append(jnp.concatenate([total[j * HEAD : (j + 1) * HEAD, HEAD:], norm], axis=0))
    first = feature[4] == 0
    keep[...] = jnp.where(first, slabs[0], slabs[1])
    give[...] = jnp.where(first, slabs[1], slabs[0])


def late_memory(feature, acc, far_a, far_b, w_key, w_value, scale):
    per_head, seg_len, _ = acc.shape
    half, width = far_a.shape
    part = pl.BlockSpec((width, HEAD), lambda h, f: (f[3], h))
    whole = pl.BlockSpec((half, width), lambda h, f: (0, 0))
    return pl.pallas_call(
        late_kernel,
        grid_spec=pltpu.PrefetchScalarGridSpec(
            num_scalar_prefetch=1,
            grid=(per_head,),
            in_specs=[
                pl.BlockSpec((None, seg_len, 2 * HEAD), lambda h, f: (h, 0, 0)),
                whole,
                whole,
                part,
                part,
                pl.BlockSpec((None, 8, seg_len), lambda h, f: (h, 0, 0)),
            ],
            out_specs=[pl.BlockSpec((None, SLAB, HEAD), lambda h, f: (h, 0, 0))] * 2,
        ),
        out_shape=[jax.ShapeDtypeStruct((per_head, SLAB, HEAD), jnp.float32)] * 2,
        cost_estimate=pl.CostEstimate(
            flops=2 * seg_len * width * per_head * 2 * HEAD, bytes_accessed=0, transcendentals=0
        ),
        compiler_params=pltpu.CompilerParams(vmem_limit_bytes=20 << 20),
        name="late",
    )(feature, acc, far_a, far_b, w_key, w_value, scale)


def tie(array, *others):
    return lax.optimization_barrier((array,) + others)[0]


def add_over_sp(keep, give):
    total = keep + swap(give, "sp", 1)
    bit = 2
    while bit < lax.axis_size("sp"):
        wire = lax.optimization_barrier(total.astype(jnp.bfloat16))
        total = wire.astype(jnp.float32) + swap(wire, "sp", bit).astype(jnp.float32)
        bit *= 2
    return lax.optimization_barrier(total.astype(jnp.bfloat16))


def read_kernel(place, *refs):
    seq_count, _, _ = refs[-4].shape
    slabs, query = refs[:-4], refs[-4]
    matrix_out, norm_out, read_out = refs[-3:]
    per_head = matrix_out.shape[2]
    core = place[0]
    for b in range(seq_count):
        for i in range(2):
            slab = slabs[2 * b + i]
            j = core if i == 0 else 1 - core
            for h in range(per_head):
                matrix_out[b, j, h] = slab[h, :HEAD, :]
                norm_out[b, j, h : h + 1] = slab[h, HEAD:, :].astype(jnp.float32)[0:1]
    for b in range(seq_count):
        for h in range(per_head):
            q = query[b, :, h * HEAD : (h + 1) * HEAD]
            q_f = q.astype(jnp.float32)
            total = None
            for j in range(2):
                top = jnp.dot(q, matrix_out[b, j, h], preferred_element_type=jnp.float32)
                below = jnp.sum(q_f * norm_out[b, j, h : h + 1], axis=1, keepdims=True)
                part = top / jnp.maximum(jnp.abs(below), 1.0)
                total = part if total is None else total + part
            read_out[b, :, h * HEAD : (h + 1) * HEAD] = total.astype(jnp.bfloat16)


def assemble_and_read(place, slabs, query, per_head):
    seq_count, new_count, width = query.shape
    return pl.pallas_call(
        read_kernel,
        in_specs=[pl.BlockSpec(memory_space=pltpu.SMEM)]
        + [pl.BlockSpec(memory_space=pltpu.VMEM)] * (len(slabs) + 1),
        out_specs=[pl.BlockSpec(memory_space=pltpu.VMEM)] * 3,
        out_shape=[
            jax.ShapeDtypeStruct((seq_count, 2, per_head, HEAD, HEAD), jnp.bfloat16),
            jax.ShapeDtypeStruct((seq_count, 2, per_head, HEAD), jnp.float32),
            jax.ShapeDtypeStruct((seq_count, new_count, width), jnp.bfloat16),
        ],
        compiler_params=pltpu.CompilerParams(vmem_limit_bytes=8 << 20),
        name="read",
    )(place, *slabs, query)


def square_group(tokens, w_key, w_value, w_gate, forget_bias, log_shift, new_query):
    seq_count, seg_len, width = tokens.shape
    per_head = w_key.shape[1] // HEAD
    t = lax.axis_index("tp")
    s = lax.axis_index("sp")
    tp = lax.axis_size("tp")
    core = s % 2
    feature = jnp.stack([t, t ^ 1, t ^ 2, t ^ 3, core]).astype(jnp.int32)
    half = seg_len // 2

    def block(source, b, r):
        return source[b, r * half : (r + 1) * half]

    x_a = swap(block(tokens, 0, 0), "tp", 1)
    y_b = swap(block(tokens, 0, 1), "tp", 2)

    gate_rows = lax.dynamic_slice_in_dim(w_gate, t * width, width, 0)
    gate_rows = gate_rows.reshape(width, 4, tp, per_head).transpose(2, 1, 3, 0)
    gate_part = lax.dot_general(
        gate_rows.reshape(tp * 4 * per_head, width),
        tokens.reshape(seq_count * seg_len, width),
        (((1,), (1,)), ((), ())),
        preferred_element_type=jnp.float32,
    ).reshape(tp, 4 * per_head, seq_count * seg_len)
    shares = [
        swap(lax.dynamic_index_in_dim(gate_part, t ^ bit, 0, keepdims=False), "tp", bit)
        for bit in range(1, tp)
    ]
    near, far = [], []
    for b in range(seq_count):
        if b:
            held = tie(tokens, *shares)
            x_a = swap(block(held, b, 0), "tp", 1)
            y_b = swap(block(held, b, 1), "tp", 2)
        else:
            held = tie(tokens, gate_part)
        x_b = swap(block(held, b, 1), "tp", 1)
        y_a = swap(block(held, b, 0), "tp", 2)
        first = (x_a, y_b)
        if b == 0:
            shares = lax.optimization_barrier(tuple(shares) + first)[: tp - 1]
        far.append((swap(x_a, "tp", 2), swap(y_b, "tp", 1)))
        near.append((x_a, x_b, y_a, y_b))
    gates = lax.dynamic_index_in_dim(gate_part, t, 0, keepdims=False)
    for share in shares:
        gates = gates + share
    gates = gates.reshape(4, per_head, seq_count, seg_len).transpose(2, 0, 1, 3)
    bias_own = lax.dynamic_slice_in_dim(forget_bias, t * per_head, per_head, 1)
    weights, totals = decay(gates, bias_own, log_shift)
    tops = jnp.stack([totals, jnp.max(weights, axis=-1)])
    every = lax.all_gather(tops, "sp")
    every_total, every_top = every[:, 0], every[:, 1]
    sources = jnp.arange(every_total.shape[0])
    direction = jnp.arange(2)[None, None, None, :, None]
    later, sooner = sources[None, :] > sources[:, None], sources[None, :] < sources[:, None]
    counted = jnp.where(direction == 0, later[..., None, None, None], sooner[..., None, None, None])
    every_passed = jnp.sum(jnp.where(counted, every_total[None], 0.0), axis=1)
    cache_max = jnp.maximum(jnp.sum(every_total, axis=0), jnp.max(every_top + every_passed, axis=0))
    passed = lax.dynamic_index_in_dim(every_passed, s, 0, keepdims=False)
    scale = jnp.exp(weights + (passed - cache_max)[..., None]) * HEAD ** (-0.5)
    scale = scale.transpose(0, 2, 1, 3)
    scale = jnp.concatenate([scale, jnp.zeros((seq_count, per_head, 6, seg_len), jnp.float32)], axis=2)

    slabs = []
    for b in range(seq_count):
        blocks = [tie(part, *slabs) for part in near[b]] if slabs else near[b]
        acc = early_projection(b, feature, tokens, blocks, w_key, w_value)
        keep, give = late_memory(feature, acc, *far[b], w_key, w_value, scale[b])
        mine = add_over_sp(keep, give)
        slabs += [mine, swap(mine, "sp", 1)]

    place = core.astype(jnp.int32)[None]
    cache_matrix, norm, first_read = assemble_and_read(place, slabs, new_query, per_head)
    return (cache_matrix, norm, cache_max, first_read)


def solution(mesh):
    def on_device(tokens, w_key, *rest):
        square = mesh.shape["tp"] == 4 and mesh.shape["sp"] == 2 * (w_key.shape[1] // HEAD)
        return (square_group if square else any_mesh)(tokens, w_key, *rest)

    return jax.shard_map(
        on_device,
        mesh=mesh,
        in_specs=(
            P(None, "sp", "tp"),
            P(None, "tp"),
            P(None, "tp"),
            P(),
            P(),
            P(None, None, "tp", "sp"),
            P(None, "sp", "tp"),
        ),
        out_specs=(
            P(None, None, "tp", None, None),
            P(None, None, "tp", None),
            P(None, None, "tp"),
            P(None, "sp", "tp"),
        ),
        check_vma=False,
    )
```

```python
import functools

import jax
import jax.numpy as jnp
from jax import lax
from jax.experimental import pallas as pl
from jax.experimental.pallas import tpu as pltpu
from jax.sharding import PartitionSpec as P


HEAD = 128
SLAB = HEAD + 8


def combined_all(array, axis, combine):
    everything = jax.tree.map(lambda part: lax.all_gather(part, axis), array)
    leading = jax.tree.map(lambda part: part[0], everything)

    def lap(k, so_far):
        return combine(so_far, jax.tree.map(lambda part: part[k], everything))

    return lax.fori_loop(1, lax.axis_size(axis), lap, leading)


def joint_max(earlier, latter):
    memory_a, norm_a, high_a = earlier
    memory_b, norm_b, high_b = latter
    highest = jnp.maximum(high_a, high_b)
    carried = jnp.exp(high_a - highest)
    own_part = jnp.exp(high_b - highest)
    memory = memory_a * carried[..., None, None] + memory_b * own_part[..., None, None]
    norm_sum = norm_a * carried[..., None] + norm_b * own_part[..., None]
    return (memory, norm_sum, highest)


def any_mesh(tokens, w_key, w_value, w_gate, forget_bias, log_shift, new_query):
    seq_count, seg_len, _ = tokens.shape
    per_head = w_key.shape[1] // HEAD
    row_count = seq_count * seg_len
    first_head = lax.axis_index("tp") * per_head
    gate_cols = lax.dynamic_slice_in_dim(w_gate, first_head, per_head, 2).reshape(
        w_gate.shape[0], 4 * per_head
    )
    bias_own = lax.dynamic_slice_in_dim(forget_bias, first_head, per_head, 1)
    piece = lax.all_gather(tokens, "tp", axis=2, tiled=True)
    piece_width = piece.shape[2]
    flat_piece = piece.reshape(row_count, piece_width)
    key_sum = jnp.dot(flat_piece, w_key, preferred_element_type=jnp.float32)
    value_sum = jnp.dot(flat_piece, w_value, preferred_element_type=jnp.float32)
    gate_sum = jnp.dot(flat_piece, gate_cols, preferred_element_type=jnp.float32)
    key_rows = key_sum.astype(jnp.bfloat16).reshape(seq_count, seg_len, per_head, HEAD)
    value_rows = value_sum.astype(jnp.bfloat16).reshape(seq_count, seg_len, per_head, HEAD)
    gates = gate_sum.reshape(seq_count, seg_len, 4, per_head).transpose(0, 2, 3, 1)
    weights, totals = decay(gates, bias_own, log_shift)
    local_top = jnp.max(weights, axis=-1)
    scale_now = jnp.exp(weights - local_top[..., None])
    key_f = key_rows.astype(jnp.float32).transpose(0, 2, 1, 3) * HEAD ** (-0.5)
    value_f = value_rows.astype(jnp.float32).transpose(0, 2, 1, 3)
    weighted = scale_now[..., None] * key_f[:, None]
    memory = jnp.einsum("bjhld,bhle->bjhde", weighted, value_f, precision=lax.Precision.HIGHEST)
    norm_sum = jnp.sum(weighted, axis=3)
    every_total = lax.all_gather(totals[None], "sp", axis=0, tiled=True)
    my_index = lax.axis_index("sp")
    sources = jnp.arange(every_total.shape[0])[:, None, None, None]
    direction = jnp.arange(2)[None, None, :, None]
    counted = jnp.where(direction == 0, sources > my_index, sources < my_index)
    passed = jnp.sum(jnp.where(counted, every_total, 0.0), axis=0)
    total_all = jnp.sum(every_total, axis=0)
    memory_all, norm_all, top_all = combined_all(
        (memory, norm_sum, local_top + passed), "sp", joint_max
    )
    cache_max = jnp.maximum(total_all, top_all)
    rescale = jnp.exp(top_all - cache_max)
    cache_matrix = (memory_all * rescale[..., None, None]).astype(jnp.bfloat16)
    cache_norm = norm_all * rescale[..., None]
    new_count = new_query.shape[1]
    queries = new_query.reshape(seq_count, new_count, per_head, HEAD)
    numerator = jnp.einsum(
        "bthd,bjhde->bjthe", queries, cache_matrix, preferred_element_type=jnp.float32
    )
    denominator = jnp.einsum(
        "bthd,bjhd->bjth", queries.astype(jnp.float32), cache_norm, precision=lax.Precision.HIGHEST
    )
    divisor = jnp.maximum(jnp.abs(denominator), 1.0)
    first_read = jnp.sum(numerator / divisor[..., None], axis=1)
    first_read = first_read.reshape(seq_count, new_count, per_head * HEAD).astype(jnp.bfloat16)
    return (cache_matrix, cache_norm, cache_max, first_read)


def decay(gates, bias_own, log_shift):
    input_fwd = gates[:, 0] + log_shift[:, 0]
    forget_fwd = jax.nn.log_sigmoid(gates[:, 1] + bias_own[0][None, :, None]) + log_shift[:, 1]
    input_bwd = gates[:, 2] + log_shift[:, 2]
    forget_bwd = jax.nn.log_sigmoid(gates[:, 3] + bias_own[1][None, :, None]) + log_shift[:, 3]
    climb = jnp.cumsum(jnp.stack([forget_fwd, forget_bwd], axis=1), axis=-1)
    totals = climb[..., -1]
    weight_fwd = totals[:, 0, :, None] - climb[:, 0] + input_fwd
    weight_bwd = climb[:, 1] - forget_bwd + input_bwd
    return jnp.stack([weight_fwd, weight_bwd], axis=1), totals


def swap(array, axis, bit):
    size = lax.axis_size(axis)
    return lax.ppermute(array, axis, [(i, i ^ bit) for i in range(size)])


def head_weights(w_key, w_value, block, width, h):
    rows = pl.ds(pl.multiple_of(block * width, width), width)
    cols = slice(h * HEAD, (h + 1) * HEAD)
    return jnp.concatenate([w_key[rows, cols], w_value[rows, cols]], axis=1)


def stacked(parts):
    values = [part[...] for part in parts]
    return values[0] if len(values) == 1 else jnp.concatenate(values, axis=0)


def early_kernel(seq, cut, feature, own, *refs):
    over_x, over_y = refs[: cut + 1], refs[cut + 1 : 2 * cut + 2]
    w_key, w_value, acc = refs[2 * cut + 2 :]
    half, width = over_x[cut].shape
    for h in range(acc.shape[0]):
        pairs = [head_weights(w_key, w_value, feature[j], width, h) for j in range(3)]
        for r, (part_x, part_y) in enumerate(
            ((over_x[:cut], over_y[:1]), (over_x[cut:], over_y[1:]))
        ):
            rows = pl.ds(r * half, half)
            total = jnp.dot(own[seq, rows, :], pairs[0], preferred_element_type=jnp.float32)
            total += jnp.dot(stacked(part_x), pairs[1], preferred_element_type=jnp.float32)
            total += jnp.dot(stacked(part_y), pairs[2], preferred_element_type=jnp.float32)
            acc[h, rows, :] = total


def in_vmem(count):
    return [pl.BlockSpec(memory_space=pltpu.SMEM)] + [pl.BlockSpec(memory_space=pltpu.VMEM)] * count


def early_projection(seq, feature, tokens, over_x, over_y, w_key, w_value):
    seg_len = tokens.shape[1]
    per_head = w_key.shape[1] // HEAD
    cut = len(over_x) - 1
    return pl.pallas_call(
        functools.partial(early_kernel, seq, cut),
        in_specs=in_vmem(2 * cut + 5),
        out_specs=pl.BlockSpec(memory_space=pltpu.VMEM),
        out_shape=jax.ShapeDtypeStruct((per_head, seg_len, 2 * HEAD), jnp.float32),
        compiler_params=pltpu.CompilerParams(vmem_limit_bytes=8 << 20),
        name="early",
    )(feature, tokens, *over_x, *over_y, w_key, w_value)


def late_kernel(heads, groups, before, last, feature, acc, *refs):
    count = sum(len(group) for group in groups)
    far, (w_key, w_value, scale), rest = refs[:count], refs[count : count + 3], refs[count + 3 :]
    width = far[0].shape[1]
    for h in heads:
        pair = head_weights(w_key, w_value, feature[3], width, h)
        total = rest[0][h] if before else None
        used = 0
        for starts in groups:
            pieces = far[used : used + len(starts)]
            used += len(starts)
            spans = [pl.ds(lo, piece.shape[0]) for lo, piece in zip(starts, pieces)]
            base = jnp.concatenate([acc[h, span, :] for span in spans], axis=0)
            now = jnp.concatenate([scale[h, :, span] for span in spans], axis=1)
            kv = base + jnp.dot(stacked(pieces), pair, preferred_element_type=jnp.float32)
            kv = kv.astype(jnp.bfloat16)
            keys_t = kv[:, :HEAD].astype(jnp.float32).T
            high = now.astype(jnp.bfloat16)
            low = (now - high.astype(jnp.float32)).astype(jnp.bfloat16)
            left = jnp.concatenate(
                [
                    (keys_t * now[0:1]).astype(jnp.bfloat16),
                    (keys_t * now[1:2]).astype(jnp.bfloat16),
                    jnp.concatenate([high, low], axis=0),
                ],
                axis=0,
            )
            part = jnp.dot(left, kv, preferred_element_type=jnp.float32)
            total = part if total is None else total + part
        if not last:
            rest[-1][h] = total
            continue
        slabs = []
        for j in range(2):
            norm = total[2 * HEAD + j : 2 * HEAD + j + 1, :HEAD]
            norm = norm + total[2 * HEAD + 8 + j : 2 * HEAD + 8 + j + 1, :HEAD]
            norm = jnp.broadcast_to(norm, (SLAB - HEAD, HEAD))
            slabs.append(jnp.concatenate([total[j * HEAD : (j + 1) * HEAD, HEAD:], norm], axis=0))
        first = feature[4] == 0
        keep, give = rest[-2:]
        keep[h - heads[0]] = jnp.where(first, slabs[0], slabs[1])
        give[h - heads[0]] = jnp.where(first, slabs[1], slabs[0])


def late_memory(heads, groups, before, last, feature, acc, w_key, w_value, scale):
    starts = tuple(tuple(lo for lo, _ in group) for group in groups)
    far = [piece for group in groups for _, piece in group]
    extra = [] if before is None else [before]
    if last:
        shapes = [jax.ShapeDtypeStruct((len(heads), SLAB, HEAD), jnp.float32)] * 2
    else:
        shapes = [jax.ShapeDtypeStruct((len(heads), 2 * HEAD + 16, 2 * HEAD), jnp.float32)]
    return pl.pallas_call(
        functools.partial(late_kernel, heads, starts, bool(extra), last),
        in_specs=in_vmem(4 + len(far) + len(extra)),
        out_specs=[pl.BlockSpec(memory_space=pltpu.VMEM)] * len(shapes),
        out_shape=shapes,
        compiler_params=pltpu.CompilerParams(vmem_limit_bytes=8 << 20),
        name="late",
    )(feature, acc, *far, w_key, w_value, scale, *extra)


def tie(array, *others):
    return lax.optimization_barrier((array,) + others)[0]


def add_over_sp(keep, give):
    halfway = []
    total = keep + swap(give, "sp", 1)
    bit = 2
    while bit < lax.axis_size("sp"):
        wire = lax.optimization_barrier(total.astype(jnp.bfloat16))
        halfway.append(wire)
        total = wire.astype(jnp.float32) + swap(wire, "sp", bit).astype(jnp.float32)
        bit *= 2
    return lax.optimization_barrier(total.astype(jnp.bfloat16)), halfway[-1]


def read_kernel(layout, place, *refs):
    seq_count, _, _ = refs[-4].shape
    slabs, query = refs[:-4], refs[-4]
    matrix_out, norm_out, read_out = refs[-3:]
    per_head = matrix_out.shape[2]
    core = place[0]
    for slab, (b, i, heads) in zip(slabs, layout):
        j = core if i == 0 else 1 - core
        for k, h in enumerate(heads):
            matrix_out[b, j, h] = slab[k, :HEAD, :]
            norm_out[b, j, h : h + 1] = slab[k, HEAD:, :].astype(jnp.float32)[0:1]
    for b in range(seq_count):
        for h in range(per_head):
            q = query[b, :, h * HEAD : (h + 1) * HEAD]
            q_f = q.astype(jnp.float32)
            total = None
            for j in range(2):
                top = jnp.dot(q, matrix_out[b, j, h], preferred_element_type=jnp.float32)
                below = jnp.sum(q_f * norm_out[b, j, h : h + 1], axis=1, keepdims=True)
                part = top / jnp.maximum(jnp.abs(below), 1.0)
                total = part if total is None else total + part
            read_out[b, :, h * HEAD : (h + 1) * HEAD] = total.astype(jnp.bfloat16)


def assemble_and_read(place, layout, slabs, query, per_head):
    seq_count, new_count, width = query.shape
    return pl.pallas_call(
        functools.partial(read_kernel, layout),
        in_specs=[pl.BlockSpec(memory_space=pltpu.SMEM)]
        + [pl.BlockSpec(memory_space=pltpu.VMEM)] * (len(slabs) + 1),
        out_specs=[pl.BlockSpec(memory_space=pltpu.VMEM)] * 3,
        out_shape=[
            jax.ShapeDtypeStruct((seq_count, 2, per_head, HEAD, HEAD), jnp.bfloat16),
            jax.ShapeDtypeStruct((seq_count, 2, per_head, HEAD), jnp.float32),
            jax.ShapeDtypeStruct((seq_count, new_count, width), jnp.bfloat16),
        ],
        compiler_params=pltpu.CompilerParams(vmem_limit_bytes=8 << 20),
        name="read",
    )(place, *slabs, query)


def square_group(tokens, w_key, w_value, w_gate, forget_bias, log_shift, new_query):
    seq_count, seg_len, width = tokens.shape
    per_head = w_key.shape[1] // HEAD
    t = lax.axis_index("tp")
    s = lax.axis_index("sp")
    tp = lax.axis_size("tp")
    core = s % 2
    feature = jnp.stack([t, t ^ 1, t ^ 2, t ^ 3, core]).astype(jnp.int32)
    half = seg_len // 2

    small = half - HEAD if half % HEAD == 0 and half > HEAD else half
    cuts = [[(0, half)]] * (seq_count - 1) + [[(0, small), (small, half)][: 1 + (small < half)]]

    def lead(source, b):
        out = []
        for lo, hi in cuts[b]:
            x_a = swap(source[b, lo:hi], "tp", 1)
            y_b = swap(source[b, half + lo : half + hi], "tp", 2)
            out.append((x_a, y_b))
        return out

    first = lead(tokens, 0)

    gate_rows = lax.dynamic_slice_in_dim(w_gate, t * width, width, 0)
    gate_rows = gate_rows.reshape(width, 4, tp, per_head).transpose(2, 1, 3, 0)
    gate_part = lax.dot_general(
        gate_rows.reshape(tp * 4 * per_head, width),
        tokens.reshape(seq_count * seg_len, width),
        (((1,), (1,)), ((), ())),
        preferred_element_type=jnp.float32,
    ).reshape(tp, 4 * per_head, seq_count * seg_len)
    shares = [
        swap(lax.dynamic_index_in_dim(gate_part, t ^ bit, 0, keepdims=False), "tp", bit)
        for bit in range(1, tp)
    ]
    held = tie(tokens, gate_part)
    over_x, over_y, far = [], [], []
    for b in range(seq_count):
        if b:
            first = lead(held, b)
        x_b = swap(held[b, half:], "tp", 1)
        y_a = swap(held[b, :half], "tp", 2)
        if b == 0:
            shares = lax.optimization_barrier(tuple(shares) + first[0])[: tp - 1]
        far.append([])
        for x_a, y_b in first:
            far[b].append((swap(x_a, "tp", 2), swap(y_b, "tp", 1)))
        over_x.append([pair[0] for pair in first] + [x_b])
        over_y.append([y_a] + [pair[1] for pair in first])
    gates = lax.dynamic_index_in_dim(gate_part, t, 0, keepdims=False)
    for share in shares:
        gates = gates + share
    gates = gates.reshape(4, per_head, seq_count, seg_len).transpose(2, 0, 1, 3)
    bias_own = lax.dynamic_slice_in_dim(forget_bias, t * per_head, per_head, 1)
    weights, totals = decay(gates, bias_own, log_shift)
    tops = jnp.stack([totals, jnp.max(weights, axis=-1)])
    every = lax.all_gather(tops, "sp")
    every_total, every_top = every[:, 0], every[:, 1]
    sources = jnp.arange(every_total.shape[0])
    direction = jnp.arange(2)[None, None, None, :, None]
    later, sooner = sources[None, :] > sources[:, None], sources[None, :] < sources[:, None]
    counted = jnp.where(direction == 0, later[..., None, None, None], sooner[..., None, None, None])
    every_passed = jnp.sum(jnp.where(counted, every_total[None], 0.0), axis=1)
    cache_max = jnp.maximum(jnp.sum(every_total, axis=0), jnp.max(every_top + every_passed, axis=0))
    passed = lax.dynamic_index_in_dim(every_passed, s, 0, keepdims=False)
    scale = jnp.exp(weights + (passed - cache_max)[..., None]) * HEAD ** (-0.5)
    scale = scale.transpose(0, 2, 1, 3)
    scale = jnp.concatenate([scale, jnp.zeros((seq_count, per_head, 6, seg_len), jnp.float32)], axis=2)

    slabs, layout = [], []
    for b in range(seq_count):
        seen_x, seen_y = over_x[b], over_y[b]
        if slabs:
            seen_x = [tie(part, halfway) for part in seen_x]
            seen_y = [tie(part, halfway) for part in seen_y]
        acc = early_projection(b, feature, tokens, seen_x, seen_y, w_key, w_value)
        shared = (feature, acc, w_key, w_value, scale[b])
        before = None
        *sooner, (far_a, far_b) = far[b]
        every = tuple(range(per_head))
        for (lo, _), (part_a, part_b) in zip(cuts[b], sooner):
            part_a, part_b = tie(part_a, *slabs), tie(part_b, *slabs)
            groups = [[(lo, part_a)], [(half + lo, part_b)]]
            (before,) = late_memory(every, groups, before, False, *shared)
        lo = cuts[b][-1][0]
        ahead = slabs if before is None else slabs + [before]
        if ahead:
            far_a, far_b = tie(far_a, *ahead), tie(far_b, *ahead)
        groups = [[(lo, far_a)], [(half + lo, far_b)]]
        if sooner:
            groups = [groups[0] + groups[1]]
        parts = 2 if b == seq_count - 1 else 1
        own = []
        for k in range(parts):
            heads = every[per_head * k // parts : per_head * (k + 1) // parts]
            keep, give = late_memory(heads, groups, before, True, *shared)
            mine, halfway = add_over_sp(keep, give)
            own += [mine, swap(mine, "sp", 1)]
            layout += [(b, 0, heads), (b, 1, heads)]
        slabs += own

    place = core.astype(jnp.int32)[None]
    cache_matrix, norm, first_read = assemble_and_read(place, layout, slabs, new_query, per_head)
    return (cache_matrix, norm, cache_max, first_read)


def solution(mesh):
    def on_device(tokens, w_key, *rest):
        square = mesh.shape["tp"] == 4 and mesh.shape["sp"] == 2 * (w_key.shape[1] // HEAD)
        return (square_group if square else any_mesh)(tokens, w_key, *rest)

    return jax.shard_map(
        on_device,
        mesh=mesh,
        in_specs=(
            P(None, "sp", "tp"),
            P(None, "tp"),
            P(None, "tp"),
            P(),
            P(),
            P(None, None, "tp", "sp"),
            P(None, "sp", "tp"),
        ),
        out_specs=(
            P(None, None, "tp", None, None),
            P(None, None, "tp", None),
            P(None, None, "tp"),
            P(None, "sp", "tp"),
        ),
        check_vma=False,
    )
```

```python
import functools

import jax
import jax.numpy as jnp
from jax import lax
from jax.experimental import pallas as pl
from jax.experimental.pallas import tpu as pltpu
from jax.sharding import PartitionSpec as P


HEAD = 128
SLAB = HEAD + 8


def combined_all(array, axis, combine):
    everything = jax.tree.map(lambda part: lax.all_gather(part, axis), array)
    leading = jax.tree.map(lambda part: part[0], everything)

    def lap(k, so_far):
        return combine(so_far, jax.tree.map(lambda part: part[k], everything))

    return lax.fori_loop(1, lax.axis_size(axis), lap, leading)


def joint_max(earlier, latter):
    memory_a, norm_a, high_a = earlier
    memory_b, norm_b, high_b = latter
    highest = jnp.maximum(high_a, high_b)
    carried = jnp.exp(high_a - highest)
    own_part = jnp.exp(high_b - highest)
    memory = memory_a * carried[..., None, None] + memory_b * own_part[..., None, None]
    norm_sum = norm_a * carried[..., None] + norm_b * own_part[..., None]
    return (memory, norm_sum, highest)


def any_mesh(tokens, w_key, w_value, w_gate, forget_bias, log_shift, new_query):
    seq_count, seg_len, _ = tokens.shape
    per_head = w_key.shape[1] // HEAD
    row_count = seq_count * seg_len
    first_head = lax.axis_index("tp") * per_head
    gate_cols = lax.dynamic_slice_in_dim(w_gate, first_head, per_head, 2).reshape(
        w_gate.shape[0], 4 * per_head
    )
    bias_own = lax.dynamic_slice_in_dim(forget_bias, first_head, per_head, 1)
    piece = lax.all_gather(tokens, "tp", axis=2, tiled=True)
    piece_width = piece.shape[2]
    flat_piece = piece.reshape(row_count, piece_width)
    key_sum = jnp.dot(flat_piece, w_key, preferred_element_type=jnp.float32)
    value_sum = jnp.dot(flat_piece, w_value, preferred_element_type=jnp.float32)
    gate_sum = jnp.dot(flat_piece, gate_cols, preferred_element_type=jnp.float32)
    key_rows = key_sum.astype(jnp.bfloat16).reshape(seq_count, seg_len, per_head, HEAD)
    value_rows = value_sum.astype(jnp.bfloat16).reshape(seq_count, seg_len, per_head, HEAD)
    gates = gate_sum.reshape(seq_count, seg_len, 4, per_head).transpose(0, 2, 3, 1)
    weights, totals = decay(gates, bias_own, log_shift)
    local_top = jnp.max(weights, axis=-1)
    scale_now = jnp.exp(weights - local_top[..., None])
    key_f = key_rows.astype(jnp.float32).transpose(0, 2, 1, 3) * HEAD ** (-0.5)
    value_f = value_rows.astype(jnp.float32).transpose(0, 2, 1, 3)
    weighted = scale_now[..., None] * key_f[:, None]
    memory = jnp.einsum("bjhld,bhle->bjhde", weighted, value_f, precision=lax.Precision.HIGHEST)
    norm_sum = jnp.sum(weighted, axis=3)
    every_total = lax.all_gather(totals[None], "sp", axis=0, tiled=True)
    my_index = lax.axis_index("sp")
    sources = jnp.arange(every_total.shape[0])[:, None, None, None]
    direction = jnp.arange(2)[None, None, :, None]
    counted = jnp.where(direction == 0, sources > my_index, sources < my_index)
    passed = jnp.sum(jnp.where(counted, every_total, 0.0), axis=0)
    total_all = jnp.sum(every_total, axis=0)
    memory_all, norm_all, top_all = combined_all(
        (memory, norm_sum, local_top + passed), "sp", joint_max
    )
    cache_max = jnp.maximum(total_all, top_all)
    rescale = jnp.exp(top_all - cache_max)
    cache_matrix = (memory_all * rescale[..., None, None]).astype(jnp.bfloat16)
    cache_norm = norm_all * rescale[..., None]
    new_count = new_query.shape[1]
    queries = new_query.reshape(seq_count, new_count, per_head, HEAD)
    numerator = jnp.einsum(
        "bthd,bjhde->bjthe", queries, cache_matrix, preferred_element_type=jnp.float32
    )
    denominator = jnp.einsum(
        "bthd,bjhd->bjth", queries.astype(jnp.float32), cache_norm, precision=lax.Precision.HIGHEST
    )
    divisor = jnp.maximum(jnp.abs(denominator), 1.0)
    first_read = jnp.sum(numerator / divisor[..., None], axis=1)
    first_read = first_read.reshape(seq_count, new_count, per_head * HEAD).astype(jnp.bfloat16)
    return (cache_matrix, cache_norm, cache_max, first_read)


def decay(gates, bias_own, log_shift):
    input_fwd = gates[:, 0] + log_shift[:, 0]
    forget_fwd = jax.nn.log_sigmoid(gates[:, 1] + bias_own[0][None, :, None]) + log_shift[:, 1]
    input_bwd = gates[:, 2] + log_shift[:, 2]
    forget_bwd = jax.nn.log_sigmoid(gates[:, 3] + bias_own[1][None, :, None]) + log_shift[:, 3]
    climb = jnp.cumsum(jnp.stack([forget_fwd, forget_bwd], axis=1), axis=-1)
    totals = climb[..., -1]
    weight_fwd = totals[:, 0, :, None] - climb[:, 0] + input_fwd
    weight_bwd = climb[:, 1] - forget_bwd + input_bwd
    return jnp.stack([weight_fwd, weight_bwd], axis=1), totals


def swap(array, axis, bit):
    size = lax.axis_size(axis)
    return lax.ppermute(array, axis, [(i, i ^ bit) for i in range(size)])


def head_weights(w_key, w_value, block, width, h):
    rows = pl.ds(pl.multiple_of(block * width, width), width)
    cols = slice(h * HEAD, (h + 1) * HEAD)
    return jnp.concatenate([w_key[rows, cols], w_value[rows, cols]], axis=1)


def stacked(parts):
    values = [part[...] for part in parts]
    return values[0] if len(values) == 1 else jnp.concatenate(values, axis=0)


def early_kernel(seq, cut, feature, own, *refs):
    over_x, over_y = refs[: cut + 1], refs[cut + 1 : 2 * cut + 2]
    w_key, w_value, acc = refs[2 * cut + 2 :]
    half, width = over_x[cut].shape
    for h in range(acc.shape[0]):
        pairs = [head_weights(w_key, w_value, feature[j], width, h) for j in range(3)]
        for r, (part_x, part_y) in enumerate(
            ((over_x[:cut], over_y[:1]), (over_x[cut:], over_y[1:]))
        ):
            rows = pl.ds(r * half, half)
            total = jnp.dot(own[seq, rows, :], pairs[0], preferred_element_type=jnp.float32)
            total += jnp.dot(stacked(part_x), pairs[1], preferred_element_type=jnp.float32)
            total += jnp.dot(stacked(part_y), pairs[2], preferred_element_type=jnp.float32)
            acc[h, rows, :] = total


def in_vmem(count):
    return [pl.BlockSpec(memory_space=pltpu.SMEM)] + [pl.BlockSpec(memory_space=pltpu.VMEM)] * count


def early_projection(seq, feature, tokens, over_x, over_y, w_key, w_value):
    seg_len = tokens.shape[1]
    per_head = w_key.shape[1] // HEAD
    cut = len(over_x) - 1
    return pl.pallas_call(
        functools.partial(early_kernel, seq, cut),
        in_specs=in_vmem(2 * cut + 5),
        out_specs=pl.BlockSpec(memory_space=pltpu.VMEM),
        out_shape=jax.ShapeDtypeStruct((per_head, seg_len, 2 * HEAD), jnp.float32),
        compiler_params=pltpu.CompilerParams(vmem_limit_bytes=8 << 20),
        name="early",
    )(feature, tokens, *over_x, *over_y, w_key, w_value)


def late_kernel(heads, groups, before, last, feature, acc, *refs):
    count = sum(len(group) for group in groups)
    far, (w_key, w_value, scale), rest = refs[:count], refs[count : count + 3], refs[count + 3 :]
    width = far[0].shape[1]
    for h in heads:
        pair = head_weights(w_key, w_value, feature[3], width, h)
        total = rest[0][h] if before else None
        used = 0
        for starts in groups:
            pieces = far[used : used + len(starts)]
            used += len(starts)
            spans = [pl.ds(lo, piece.shape[0]) for lo, piece in zip(starts, pieces)]
            base = jnp.concatenate([acc[h, span, :] for span in spans], axis=0)
            now = jnp.concatenate([scale[h, :, span] for span in spans], axis=1)
            kv = base + jnp.dot(stacked(pieces), pair, preferred_element_type=jnp.float32)
            kv = kv.astype(jnp.bfloat16)
            keys_t = kv[:, :HEAD].astype(jnp.float32).T
            high = now.astype(jnp.bfloat16)
            low = (now - high.astype(jnp.float32)).astype(jnp.bfloat16)
            left = jnp.concatenate(
                [
                    (keys_t * now[0:1]).astype(jnp.bfloat16),
                    (keys_t * now[1:2]).astype(jnp.bfloat16),
                    jnp.concatenate([high, low], axis=0),
                ],
                axis=0,
            )
            part = jnp.dot(left, kv, preferred_element_type=jnp.float32)
            total = part if total is None else total + part
        if not last:
            rest[-1][h] = total
            continue
        slabs = []
        for j in range(2):
            norm = total[2 * HEAD + j : 2 * HEAD + j + 1, :HEAD]
            norm = norm + total[2 * HEAD + 8 + j : 2 * HEAD + 8 + j + 1, :HEAD]
            norm = jnp.broadcast_to(norm, (SLAB - HEAD, HEAD))
            slabs.append(jnp.concatenate([total[j * HEAD : (j + 1) * HEAD, HEAD:], norm], axis=0))
        first = feature[4] == 0
        keep, give = rest[-2:]
        keep[h - heads[0]] = jnp.where(first, slabs[0], slabs[1])
        give[h - heads[0]] = jnp.where(first, slabs[1], slabs[0])


def late_memory(heads, groups, before, last, feature, acc, w_key, w_value, scale):
    starts = tuple(tuple(lo for lo, _ in group) for group in groups)
    far = [piece for group in groups for _, piece in group]
    extra = [] if before is None else [before]
    if last:
        shapes = [jax.ShapeDtypeStruct((len(heads), SLAB, HEAD), jnp.float32)] * 2
    else:
        shapes = [jax.ShapeDtypeStruct((len(heads), 2 * HEAD + 16, 2 * HEAD), jnp.float32)]
    return pl.pallas_call(
        functools.partial(late_kernel, heads, starts, bool(extra), last),
        in_specs=in_vmem(4 + len(far) + len(extra)),
        out_specs=[pl.BlockSpec(memory_space=pltpu.VMEM)] * len(shapes),
        out_shape=shapes,
        compiler_params=pltpu.CompilerParams(vmem_limit_bytes=8 << 20),
        name="late",
    )(feature, acc, *far, w_key, w_value, scale, *extra)


def tie(array, *others):
    return lax.optimization_barrier((array,) + others)[0]


def add_over_sp(keep, give):
    total = keep + swap(give, "sp", 1)
    bit = 2
    while bit < lax.axis_size("sp"):
        wire = lax.optimization_barrier(total.astype(jnp.bfloat16))
        total = wire.astype(jnp.float32) + swap(wire, "sp", bit).astype(jnp.float32)
        bit *= 2
    return lax.optimization_barrier(total.astype(jnp.bfloat16)), wire


def read_kernel(layout, place, *refs):
    seq_count, _, _ = refs[-4].shape
    slabs, query = refs[:-4], refs[-4]
    matrix_out, norm_out, read_out = refs[-3:]
    per_head = matrix_out.shape[2]
    core = place[0]
    for slab, (b, i, heads) in zip(slabs, layout):
        j = core if i == 0 else 1 - core
        for k, h in enumerate(heads):
            matrix_out[b, j, h] = slab[k, :HEAD, :]
            norm_out[b, j, h : h + 1] = slab[k, HEAD:, :].astype(jnp.float32)[0:1]
    for b in range(seq_count):
        for h in range(per_head):
            q = query[b, :, h * HEAD : (h + 1) * HEAD]
            q_f = q.astype(jnp.float32)
            total = None
            for j in range(2):
                top = jnp.dot(q, matrix_out[b, j, h], preferred_element_type=jnp.float32)
                below = jnp.sum(q_f * norm_out[b, j, h : h + 1], axis=1, keepdims=True)
                part = top / jnp.maximum(jnp.abs(below), 1.0)
                total = part if total is None else total + part
            read_out[b, :, h * HEAD : (h + 1) * HEAD] = total.astype(jnp.bfloat16)


def assemble_and_read(place, layout, slabs, query, per_head):
    seq_count, new_count, width = query.shape
    return pl.pallas_call(
        functools.partial(read_kernel, layout),
        in_specs=[pl.BlockSpec(memory_space=pltpu.SMEM)]
        + [pl.BlockSpec(memory_space=pltpu.VMEM)] * (len(slabs) + 1),
        out_specs=[pl.BlockSpec(memory_space=pltpu.VMEM)] * 3,
        out_shape=[
            jax.ShapeDtypeStruct((seq_count, 2, per_head, HEAD, HEAD), jnp.bfloat16),
            jax.ShapeDtypeStruct((seq_count, 2, per_head, HEAD), jnp.float32),
            jax.ShapeDtypeStruct((seq_count, new_count, width), jnp.bfloat16),
        ],
        compiler_params=pltpu.CompilerParams(vmem_limit_bytes=8 << 20),
        name="read",
    )(place, *slabs, query)


def square_group(tokens, w_key, w_value, w_gate, forget_bias, log_shift, new_query):
    seq_count, seg_len, width = tokens.shape
    per_head = w_key.shape[1] // HEAD
    t = lax.axis_index("tp")
    s = lax.axis_index("sp")
    tp = lax.axis_size("tp")
    core = s % 2
    feature = jnp.stack([t, t ^ 1, t ^ 2, t ^ 3, core]).astype(jnp.int32)
    half = seg_len // 2

    small = half - HEAD if half % HEAD == 0 and half > HEAD else half
    cuts = [[(0, half)]] * (seq_count - 1) + [[(0, small), (small, half)][: 1 + (small < half)]]
    if small < half and seq_count > 1:
        cuts[0] = [(0, HEAD), (HEAD, half)]

    def lead(source, b):
        out = []
        for lo, hi in cuts[b]:
            if out and b == 0:
                source = tie(source, tip)
            tip = source[b, lo:hi]
            x_a = swap(tip, "tp", 1)
            y_b = swap(source[b, half + lo : half + hi], "tp", 2)
            out.append((x_a, y_b))
        return out

    first = lead(tokens, 0)

    gate_rows = lax.dynamic_slice_in_dim(w_gate, t * width, width, 0)
    gate_rows = gate_rows.reshape(width, 4, tp, per_head).transpose(2, 1, 3, 0)
    gate_part = lax.dot_general(
        gate_rows.reshape(tp * 4 * per_head, width),
        tokens.reshape(seq_count * seg_len, width),
        (((1,), (1,)), ((), ())),
        preferred_element_type=jnp.float32,
    ).reshape(tp, 4 * per_head, seq_count * seg_len)
    shares = [
        swap(lax.dynamic_index_in_dim(gate_part, t ^ bit, 0, keepdims=False), "tp", bit)
        for bit in range(1, tp)
    ]
    held = tie(tokens, gate_part)
    over_x, over_y, far = [], [], []
    for b in range(seq_count):
        if b:
            first = lead(held, b)
        x_b = swap(held[b, half:], "tp", 1)
        y_a = swap(held[b, :half], "tp", 2)
        if b == 0:
            shares = lax.optimization_barrier(tuple(shares) + first[-1])[: tp - 1]
        far.append([])
        for x_a, y_b in first:
            far[b].append((swap(x_a, "tp", 2), swap(y_b, "tp", 1)))
        over_x.append([pair[0] for pair in first] + [x_b])
        over_y.append([y_a] + [pair[1] for pair in first])
    gates = lax.dynamic_index_in_dim(gate_part, t, 0, keepdims=False)
    for share in shares:
        gates = gates + share
    gates = gates.reshape(4, per_head, seq_count, seg_len).transpose(2, 0, 1, 3)
    bias_own = lax.dynamic_slice_in_dim(forget_bias, t * per_head, per_head, 1)
    weights, totals = decay(gates, bias_own, log_shift)
    tops = jnp.stack([totals, jnp.max(weights, axis=-1)])
    every = lax.all_gather(tops, "sp")
    every_total, every_top = every[:, 0], every[:, 1]
    sources = jnp.arange(every_total.shape[0])
    direction = jnp.arange(2)[None, None, None, :, None]
    later, sooner = sources[None, :] > sources[:, None], sources[None, :] < sources[:, None]
    counted = jnp.where(direction == 0, later[..., None, None, None], sooner[..., None, None, None])
    every_passed = jnp.sum(jnp.where(counted, every_total[None], 0.0), axis=1)
    cache_max = jnp.maximum(jnp.sum(every_total, axis=0), jnp.max(every_top + every_passed, axis=0))
    passed = lax.dynamic_index_in_dim(every_passed, s, 0, keepdims=False)
    scale = jnp.exp(weights + (passed - cache_max)[..., None]) * HEAD ** (-0.5)
    scale = scale.transpose(0, 2, 1, 3)
    scale = jnp.concatenate([scale, jnp.zeros((seq_count, per_head, 6, seg_len), jnp.float32)], axis=2)

    slabs, layout = [], []
    for b in range(seq_count):
        seen_x, seen_y = over_x[b], over_y[b]
        if slabs:
            seen_x = [tie(part, halfway) for part in seen_x]
            seen_y = [tie(part, halfway) for part in seen_y]
        acc = early_projection(b, feature, tokens, seen_x, seen_y, w_key, w_value)
        shared = (feature, acc, w_key, w_value, scale[b])
        before = None
        *sooner, (far_a, far_b) = far[b]
        every = tuple(range(per_head))
        whole = b < seq_count - 1
        for (lo, _), (part_a, part_b) in zip(cuts[b], () if whole else sooner):
            part_a, part_b = tie(part_a, *slabs), tie(part_b, *slabs)
            groups = [[(lo, part_a)], [(half + lo, part_b)]]
            (before,) = late_memory(every, groups, before, False, *shared)
        lo = cuts[b][-1][0]
        ahead = slabs if before is None else slabs + [before]
        if ahead:
            far_a, far_b = tie(far_a, *ahead), tie(far_b, *ahead)
        groups = [[(lo, far_a)], [(half + lo, far_b)]]
        if whole:
            groups = [
                [(r * half + cut[0], pair[r]) for cut, pair in zip(cuts[b], far[b])] for r in range(2)
            ]
        parts = 2 if b == seq_count - 1 and per_head > 1 else 1
        own = []
        for k in range(parts):
            heads = every[per_head * k // parts : per_head * (k + 1) // parts]
            keep, give = late_memory(heads, groups, before, True, *shared)
            mine, halfway = add_over_sp(keep, give)
            own += [mine, swap(mine, "sp", 1)]
            layout += [(b, 0, heads), (b, 1, heads)]
        slabs += own

    place = core.astype(jnp.int32)[None]
    cache_matrix, norm, first_read = assemble_and_read(place, layout, slabs, new_query, per_head)
    return (cache_matrix, norm, cache_max, first_read)


def solution(mesh):
    def on_device(tokens, w_key, *rest):
        square = mesh.shape["tp"] == 4 and mesh.shape["sp"] == 2 * (w_key.shape[1] // HEAD)
        return (square_group if square else any_mesh)(tokens, w_key, *rest)

    return jax.shard_map(
        on_device,
        mesh=mesh,
        in_specs=(
            P(None, "sp", "tp"),
            P(None, "tp"),
            P(None, "tp"),
            P(),
            P(),
            P(None, None, "tp", "sp"),
            P(None, "sp", "tp"),
        ),
        out_specs=(
            P(None, None, "tp", None, None),
            P(None, None, "tp", None),
            P(None, None, "tp"),
            P(None, "sp", "tp"),
        ),
        check_vma=False,
    )
```

```python
import functools

import jax
import jax.numpy as jnp
from jax import lax
from jax.experimental import pallas as pl
from jax.experimental.pallas import tpu as pltpu
from jax.sharding import PartitionSpec as P


HEAD = 128
SLAB = HEAD + 8


def combined_all(array, axis, combine):
    everything = jax.tree.map(lambda part: lax.all_gather(part, axis), array)
    leading = jax.tree.map(lambda part: part[0], everything)

    def lap(k, so_far):
        return combine(so_far, jax.tree.map(lambda part: part[k], everything))

    return lax.fori_loop(1, lax.axis_size(axis), lap, leading)


def joint_max(earlier, latter):
    memory_a, norm_a, high_a = earlier
    memory_b, norm_b, high_b = latter
    highest = jnp.maximum(high_a, high_b)
    carried = jnp.exp(high_a - highest)
    own_part = jnp.exp(high_b - highest)
    memory = memory_a * carried[..., None, None] + memory_b * own_part[..., None, None]
    norm_sum = norm_a * carried[..., None] + norm_b * own_part[..., None]
    return (memory, norm_sum, highest)


def any_mesh(tokens, w_key, w_value, w_gate, forget_bias, log_shift, new_query):
    seq_count, seg_len, _ = tokens.shape
    per_head = w_key.shape[1] // HEAD
    row_count = seq_count * seg_len
    first_head = lax.axis_index("tp") * per_head
    gate_cols = lax.dynamic_slice_in_dim(w_gate, first_head, per_head, 2).reshape(
        w_gate.shape[0], 4 * per_head
    )
    bias_own = lax.dynamic_slice_in_dim(forget_bias, first_head, per_head, 1)
    piece = lax.all_gather(tokens, "tp", axis=2, tiled=True)
    piece_width = piece.shape[2]
    flat_piece = piece.reshape(row_count, piece_width)
    key_sum = jnp.dot(flat_piece, w_key, preferred_element_type=jnp.float32)
    value_sum = jnp.dot(flat_piece, w_value, preferred_element_type=jnp.float32)
    gate_sum = jnp.dot(flat_piece, gate_cols, preferred_element_type=jnp.float32)
    key_rows = key_sum.astype(jnp.bfloat16).reshape(seq_count, seg_len, per_head, HEAD)
    value_rows = value_sum.astype(jnp.bfloat16).reshape(seq_count, seg_len, per_head, HEAD)
    gates = gate_sum.reshape(seq_count, seg_len, 4, per_head).transpose(0, 2, 3, 1)
    weights, totals = decay(gates, bias_own, log_shift)
    local_top = jnp.max(weights, axis=-1)
    scale_now = jnp.exp(weights - local_top[..., None])
    key_f = key_rows.astype(jnp.float32).transpose(0, 2, 1, 3) * HEAD ** (-0.5)
    value_f = value_rows.astype(jnp.float32).transpose(0, 2, 1, 3)
    weighted = scale_now[..., None] * key_f[:, None]
    memory = jnp.einsum("bjhld,bhle->bjhde", weighted, value_f, precision=lax.Precision.HIGHEST)
    norm_sum = jnp.sum(weighted, axis=3)
    every_total = lax.all_gather(totals[None], "sp", axis=0, tiled=True)
    my_index = lax.axis_index("sp")
    sources = jnp.arange(every_total.shape[0])[:, None, None, None]
    direction = jnp.arange(2)[None, None, :, None]
    counted = jnp.where(direction == 0, sources > my_index, sources < my_index)
    passed = jnp.sum(jnp.where(counted, every_total, 0.0), axis=0)
    total_all = jnp.sum(every_total, axis=0)
    memory_all, norm_all, top_all = combined_all(
        (memory, norm_sum, local_top + passed), "sp", joint_max
    )
    cache_max = jnp.maximum(total_all, top_all)
    rescale = jnp.exp(top_all - cache_max)
    cache_matrix = (memory_all * rescale[..., None, None]).astype(jnp.bfloat16)
    cache_norm = norm_all * rescale[..., None]
    new_count = new_query.shape[1]
    queries = new_query.reshape(seq_count, new_count, per_head, HEAD)
    numerator = jnp.einsum(
        "bthd,bjhde->bjthe", queries, cache_matrix, preferred_element_type=jnp.float32
    )
    denominator = jnp.einsum(
        "bthd,bjhd->bjth", queries.astype(jnp.float32), cache_norm, precision=lax.Precision.HIGHEST
    )
    divisor = jnp.maximum(jnp.abs(denominator), 1.0)
    first_read = jnp.sum(numerator / divisor[..., None], axis=1)
    first_read = first_read.reshape(seq_count, new_count, per_head * HEAD).astype(jnp.bfloat16)
    return (cache_matrix, cache_norm, cache_max, first_read)


def decay(gates, bias_own, log_shift):
    input_fwd = gates[:, 0] + log_shift[:, 0]
    forget_fwd = jax.nn.log_sigmoid(gates[:, 1] + bias_own[0][None, :, None]) + log_shift[:, 1]
    input_bwd = gates[:, 2] + log_shift[:, 2]
    forget_bwd = jax.nn.log_sigmoid(gates[:, 3] + bias_own[1][None, :, None]) + log_shift[:, 3]
    climb = jnp.cumsum(jnp.stack([forget_fwd, forget_bwd], axis=1), axis=-1)
    totals = climb[..., -1]
    weight_fwd = totals[:, 0, :, None] - climb[:, 0] + input_fwd
    weight_bwd = climb[:, 1] - forget_bwd + input_bwd
    return jnp.stack([weight_fwd, weight_bwd], axis=1), totals


def swap(array, axis, bit):
    size = lax.axis_size(axis)
    return lax.ppermute(array, axis, [(i, i ^ bit) for i in range(size)])


def norm_scales():
    count = SLAB - HEAD
    row = lax.broadcasted_iota(jnp.int32, (count, HEAD), 0)
    return jnp.exp2(row.astype(jnp.float32) / count)


def head_weights(w_key, w_value, block, width, h):
    rows = pl.ds(pl.multiple_of(block * width, width), width)
    cols = slice(h * HEAD, (h + 1) * HEAD)
    return jnp.concatenate([w_key[rows, cols], w_value[rows, cols]], axis=1)


def stacked(parts):
    values = [part[...] for part in parts]
    return values[0] if len(values) == 1 else jnp.concatenate(values, axis=0)


def early_kernel(seq, cut, feature, own, *refs):
    over_x, over_y = refs[: cut + 1], refs[cut + 1 : 2 * cut + 2]
    w_key, w_value, acc = refs[2 * cut + 2 :]
    half, width = over_x[cut].shape
    for h in range(acc.shape[0]):
        pairs = [head_weights(w_key, w_value, feature[j], width, h) for j in range(3)]
        for r, (part_x, part_y) in enumerate(
            ((over_x[:cut], over_y[:1]), (over_x[cut:], over_y[1:]))
        ):
            rows = pl.ds(r * half, half)
            total = jnp.dot(own[seq, rows, :], pairs[0], preferred_element_type=jnp.float32)
            total += jnp.dot(stacked(part_x), pairs[1], preferred_element_type=jnp.float32)
            total += jnp.dot(stacked(part_y), pairs[2], preferred_element_type=jnp.float32)
            acc[h, rows, :] = total


def in_vmem(count):
    return [pl.BlockSpec(memory_space=pltpu.SMEM)] + [pl.BlockSpec(memory_space=pltpu.VMEM)] * count


def early_projection(seq, feature, tokens, over_x, over_y, w_key, w_value):
    seg_len = tokens.shape[1]
    per_head = w_key.shape[1] // HEAD
    cut = len(over_x) - 1
    return pl.pallas_call(
        functools.partial(early_kernel, seq, cut),
        in_specs=in_vmem(2 * cut + 5),
        out_specs=pl.BlockSpec(memory_space=pltpu.VMEM),
        out_shape=jax.ShapeDtypeStruct((per_head, seg_len, 2 * HEAD), jnp.float32),
        compiler_params=pltpu.CompilerParams(vmem_limit_bytes=8 << 20),
        name="early",
    )(feature, tokens, *over_x, *over_y, w_key, w_value)


def late_kernel(heads, groups, before, last, feature, acc, *refs):
    count = sum(len(group) for group in groups)
    far, (w_key, w_value, scale), rest = refs[:count], refs[count : count + 3], refs[count + 3 :]
    width = far[0].shape[1]
    for h in heads:
        pair = head_weights(w_key, w_value, feature[3], width, h)
        total = rest[0][h] if before else None
        used = 0
        for starts in groups:
            pieces = far[used : used + len(starts)]
            used += len(starts)
            spans = [pl.ds(lo, piece.shape[0]) for lo, piece in zip(starts, pieces)]
            base = jnp.concatenate([acc[h, span, :] for span in spans], axis=0)
            now = jnp.concatenate([scale[h, :, span] for span in spans], axis=1)
            kv = base + jnp.dot(stacked(pieces), pair, preferred_element_type=jnp.float32)
            kv = kv.astype(jnp.bfloat16)
            keys_t = kv[:, :HEAD].astype(jnp.float32).T
            high = now.astype(jnp.bfloat16)
            low = (now - high.astype(jnp.float32)).astype(jnp.bfloat16)
            left = jnp.concatenate(
                [
                    (keys_t * now[0:1]).astype(jnp.bfloat16),
                    (keys_t * now[1:2]).astype(jnp.bfloat16),
                    jnp.concatenate([high, low], axis=0),
                ],
                axis=0,
            )
            part = jnp.dot(left, kv, preferred_element_type=jnp.float32)
            total = part if total is None else total + part
        if not last:
            rest[-1][h] = total
            continue
        slabs = []
        for j in range(2):
            norm = total[2 * HEAD + j : 2 * HEAD + j + 1, :HEAD]
            norm = norm + total[2 * HEAD + 8 + j : 2 * HEAD + 8 + j + 1, :HEAD]
            norm = norm * norm_scales()
            slabs.append(jnp.concatenate([total[j * HEAD : (j + 1) * HEAD, HEAD:], norm], axis=0))
        first = feature[4] == 0
        keep, give = rest[-2:]
        keep[h - heads[0]] = jnp.where(first, slabs[0], slabs[1])
        give[h - heads[0]] = jnp.where(first, slabs[1], slabs[0])


def late_memory(heads, groups, before, last, feature, acc, w_key, w_value, scale):
    starts = tuple(tuple(lo for lo, _ in group) for group in groups)
    far = [piece for group in groups for _, piece in group]
    extra = [] if before is None else [before]
    if last:
        shapes = [jax.ShapeDtypeStruct((len(heads), SLAB, HEAD), jnp.float32)] * 2
    else:
        shapes = [jax.ShapeDtypeStruct((len(heads), 2 * HEAD + 16, 2 * HEAD), jnp.float32)]
    return pl.pallas_call(
        functools.partial(late_kernel, heads, starts, bool(extra), last),
        in_specs=in_vmem(4 + len(far) + len(extra)),
        out_specs=[pl.BlockSpec(memory_space=pltpu.VMEM)] * len(shapes),
        out_shape=shapes,
        compiler_params=pltpu.CompilerParams(vmem_limit_bytes=8 << 20),
        name="late",
    )(feature, acc, *far, w_key, w_value, scale, *extra)


def tie(array, *others):
    return lax.optimization_barrier((array,) + others)[0]


def add_over_sp(keep, give):
    total = keep + swap(give, "sp", 1)
    bit = 2
    while bit < lax.axis_size("sp"):
        wire = lax.optimization_barrier(total.astype(jnp.bfloat16))
        total = wire.astype(jnp.float32) + swap(wire, "sp", bit).astype(jnp.float32)
        bit *= 2
    return lax.optimization_barrier(total.astype(jnp.bfloat16)), wire


def read_kernel(layout, place, *refs):
    seq_count, _, _ = refs[-4].shape
    slabs, query = refs[:-4], refs[-4]
    matrix_out, norm_out, read_out = refs[-3:]
    per_head = matrix_out.shape[2]
    core = place[0]
    for slab, (b, i, heads) in zip(slabs, layout):
        j = core if i == 0 else 1 - core
        for k, h in enumerate(heads):
            matrix_out[b, j, h] = slab[k, :HEAD, :]
            norm = slab[k, HEAD:, :].astype(jnp.float32) / norm_scales()
            norm_out[b, j, h : h + 1] = jnp.mean(norm, axis=0, keepdims=True)
    for b in range(seq_count):
        for h in range(per_head):
            q = query[b, :, h * HEAD : (h + 1) * HEAD]
            q_f = q.astype(jnp.float32)
            total = None
            for j in range(2):
                top = jnp.dot(q, matrix_out[b, j, h], preferred_element_type=jnp.float32)
                below = jnp.sum(q_f * norm_out[b, j, h : h + 1], axis=1, keepdims=True)
                part = top / jnp.maximum(jnp.abs(below), 1.0)
                total = part if total is None else total + part
            read_out[b, :, h * HEAD : (h + 1) * HEAD] = total.astype(jnp.bfloat16)


def assemble_and_read(place, layout, slabs, query, per_head):
    seq_count, new_count, width = query.shape
    return pl.pallas_call(
        functools.partial(read_kernel, layout),
        in_specs=[pl.BlockSpec(memory_space=pltpu.SMEM)]
        + [pl.BlockSpec(memory_space=pltpu.VMEM)] * (len(slabs) + 1),
        out_specs=[pl.BlockSpec(memory_space=pltpu.VMEM)] * 3,
        out_shape=[
            jax.ShapeDtypeStruct((seq_count, 2, per_head, HEAD, HEAD), jnp.bfloat16),
            jax.ShapeDtypeStruct((seq_count, 2, per_head, HEAD), jnp.float32),
            jax.ShapeDtypeStruct((seq_count, new_count, width), jnp.bfloat16),
        ],
        compiler_params=pltpu.CompilerParams(vmem_limit_bytes=8 << 20),
        name="read",
    )(place, *slabs, query)


def square_group(tokens, w_key, w_value, w_gate, forget_bias, log_shift, new_query):
    seq_count, seg_len, width = tokens.shape
    per_head = w_key.shape[1] // HEAD
    t = lax.axis_index("tp")
    s = lax.axis_index("sp")
    tp = lax.axis_size("tp")
    core = s % 2
    feature = jnp.stack([t, t ^ 1, t ^ 2, t ^ 3, core]).astype(jnp.int32)
    half = seg_len // 2

    small = half - HEAD if half % HEAD == 0 and half > HEAD else half
    cuts = [[(0, half)]] * (seq_count - 1) + [[(0, small), (small, half)][: 1 + (small < half)]]
    if small < half and seq_count > 1:
        cuts[0] = [(0, HEAD), (HEAD, half)]

    def lead(source, b):
        out = []
        for lo, hi in cuts[b]:
            if out and b == 0:
                source = tie(source, tip)
            tip = source[b, lo:hi]
            x_a = swap(tip, "tp", 1)
            y_b = swap(source[b, half + lo : half + hi], "tp", 2)
            out.append((x_a, y_b))
        return out

    first = lead(tokens, 0)

    gate_rows = lax.dynamic_slice_in_dim(w_gate, t * width, width, 0)
    gate_rows = gate_rows.reshape(width, 4, tp, per_head).transpose(2, 1, 3, 0)
    gate_part = lax.dot_general(
        gate_rows.reshape(tp * 4 * per_head, width),
        tokens.reshape(seq_count * seg_len, width),
        (((1,), (1,)), ((), ())),
        preferred_element_type=jnp.float32,
    ).reshape(tp, 4 * per_head, seq_count * seg_len)
    shares = [
        swap(lax.dynamic_index_in_dim(gate_part, t ^ bit, 0, keepdims=False), "tp", bit)
        for bit in range(1, tp)
    ]
    held = tie(tokens, gate_part)
    over_x, over_y, far = [], [], []
    for b in range(seq_count):
        if b:
            first = lead(held, b)
        x_b = swap(held[b, half:], "tp", 1)
        y_a = swap(held[b, :half], "tp", 2)
        if b == 0:
            shares = lax.optimization_barrier(tuple(shares) + first[-1])[: tp - 1]
        far.append([])
        for x_a, y_b in first:
            far[b].append((swap(x_a, "tp", 2), swap(y_b, "tp", 1)))
        over_x.append([pair[0] for pair in first] + [x_b])
        over_y.append([y_a] + [pair[1] for pair in first])
    gates = lax.dynamic_index_in_dim(gate_part, t, 0, keepdims=False)
    for share in shares:
        gates = gates + share
    gates = gates.reshape(4, per_head, seq_count, seg_len).transpose(2, 0, 1, 3)
    bias_own = lax.dynamic_slice_in_dim(forget_bias, t * per_head, per_head, 1)
    weights, totals = decay(gates, bias_own, log_shift)
    tops = jnp.stack([totals, jnp.max(weights, axis=-1)])
    every = lax.all_gather(tops, "sp")
    every_total, every_top = every[:, 0], every[:, 1]
    sources = jnp.arange(every_total.shape[0])
    direction = jnp.arange(2)[None, None, None, :, None]
    later, sooner = sources[None, :] > sources[:, None], sources[None, :] < sources[:, None]
    counted = jnp.where(direction == 0, later[..., None, None, None], sooner[..., None, None, None])
    every_passed = jnp.sum(jnp.where(counted, every_total[None], 0.0), axis=1)
    cache_max = jnp.maximum(jnp.sum(every_total, axis=0), jnp.max(every_top + every_passed, axis=0))
    passed = lax.dynamic_index_in_dim(every_passed, s, 0, keepdims=False)
    scale = jnp.exp(weights + (passed - cache_max)[..., None]) * HEAD ** (-0.5)
    scale = scale.transpose(0, 2, 1, 3)
    scale = jnp.concatenate([scale, jnp.zeros((seq_count, per_head, 6, seg_len), jnp.float32)], axis=2)

    slabs, layout = [], []
    for b in range(seq_count):
        seen_x, seen_y = over_x[b], over_y[b]
        if slabs:
            seen_x = [tie(part, halfway) for part in seen_x]
            seen_y = [tie(part, halfway) for part in seen_y]
        acc = early_projection(b, feature, tokens, seen_x, seen_y, w_key, w_value)
        shared = (feature, acc, w_key, w_value, scale[b])
        before = None
        *sooner, (far_a, far_b) = far[b]
        every = tuple(range(per_head))
        whole = b < seq_count - 1
        for (lo, _), (part_a, part_b) in zip(cuts[b], () if whole else sooner):
            part_a, part_b = tie(part_a, *slabs), tie(part_b, *slabs)
            groups = [[(lo, part_a)], [(half + lo, part_b)]]
            (before,) = late_memory(every, groups, before, False, *shared)
        lo = cuts[b][-1][0]
        ahead = slabs if before is None else slabs + [before]
        if ahead:
            far_a, far_b = tie(far_a, *ahead), tie(far_b, *ahead)
        groups = [[(lo, far_a)], [(half + lo, far_b)]]
        if whole:
            groups = [
                [(r * half + cut[0], pair[r]) for cut, pair in zip(cuts[b], far[b])] for r in range(2)
            ]
        parts = 2 if b == seq_count - 1 and per_head > 1 else 1
        own = []
        for k in range(parts):
            heads = every[per_head * k // parts : per_head * (k + 1) // parts]
            keep, give = late_memory(heads, groups, before, True, *shared)
            mine, halfway = add_over_sp(keep, give)
            own += [mine, swap(mine, "sp", 1)]
            layout += [(b, 0, heads), (b, 1, heads)]
        slabs += own

    place = core.astype(jnp.int32)[None]
    cache_matrix, norm, first_read = assemble_and_read(place, layout, slabs, new_query, per_head)
    return (cache_matrix, norm, cache_max, first_read)


def solution(mesh):
    def on_device(tokens, w_key, *rest):
        square = mesh.shape["tp"] == 4 and mesh.shape["sp"] == 2 * (w_key.shape[1] // HEAD)
        return (square_group if square else any_mesh)(tokens, w_key, *rest)

    return jax.shard_map(
        on_device,
        mesh=mesh,
        in_specs=(
            P(None, "sp", "tp"),
            P(None, "tp"),
            P(None, "tp"),
            P(),
            P(),
            P(None, None, "tp", "sp"),
            P(None, "sp", "tp"),
        ),
        out_specs=(
            P(None, None, "tp", None, None),
            P(None, None, "tp", None),
            P(None, None, "tp"),
            P(None, "sp", "tp"),
        ),
        check_vma=False,
    )
```
